512 devices in a mesh: ep: 128 (over z, x, core), tp: 4 (over y).
Axes of the slice: x: 4, y: 4, z: 16, core: 2. Of those that a mesh axis runs over, the one named last changes fastest.
Arguments:
- hidden: bfloat16 [512, 2048], P('ep'), may hold values from -6 to 6
- attn_gain: float32 [2048], replicated, may hold values from 0.3 to 3
- query_weight: bfloat16 [2048, 2048], P('ep', 'tp'), may hold values from -0.125 to 0.125
- head_bias: float32 [16], replicated, may hold values from -10 to -4
- key_cache: bfloat16 [512, 4, 1024, 128], P('ep', 'tp'), may hold values from -6 to 6
- value_cache: bfloat16 [512, 4, 1024, 128], P('ep', 'tp'), may hold values from -7 to 7
- lengths: int32 [512], P('ep'), may hold values from 256 to 1024, as said below
- out_weight: bfloat16 [2048, 2048], P('tp', 'ep'), may hold values from -0.125 to 0.125
- moe_gain: float32 [2048], replicated, may hold values from 0.1 to 1.9
- route_group: int32 [512], P('ep'), may hold values from 0 to 3, as said below
- route_inner: int32 [512, 2], P('ep'), may hold values from 0 to 31, as said below
- route_weight: bfloat16 [512, 2], P('ep'), may hold values from 0.25 to 1
- gate_w: bfloat16 [128, 2048, 768], P('ep', None, 'tp'), may hold values from -0.125 to 0.125
- up_w: bfloat16 [128, 2048, 768], P('ep', None, 'tp'), may hold values from -0.125 to 0.125
- down_w: bfloat16 [128, 768, 2048], P('ep', 'tp'), may hold values from -0.21875 to 0.21875
Outputs:
- mixed: bfloat16 [512, 2048], P('ep', 'tp')
The draws below stay inside these ranges and needn't reach their ends.
Inputs may be any that keep to these rules, and one draw needn't show every extreme that they name: `lengths`: some sequence has length 1024 in every draw. Within the rows of one device (aligned blocks of 4 rows) no expert route_group * 32 + route_inner is named twice; one expert is named in every block. `route_inner`: the 2 entries of a row differ.
All inputs are finite; a program needn't handle non-finite values.
Results may differ from the reference program's by a relative error of at most 0.013.
Values may be sent and summed in bfloat16 or wider, within the bound.
A program may use at most 64 MiB of HBM per device.

```python
import math
import jax
import jax.numpy as jnp
from jax import lax

D = 2048
HEADS = 16
KV_HEADS = 4
HEAD_SIZE = 128
FF_EXP = 768
TOPK = 2
SEQ_DEV = 4
CACHE = 1024
TOKENS = 512
EXPERTS = 128
GROUPS = 4
GROUP_SIZE = 32
N_EP = 128
N_TP = 4


def routing_tables(key):
    base = jax.random.fold_in(key, 7001)
    key_hot, key_perm, key_pairs, key_star = jax.random.split(base, 4)
    blocks = TOKENS // SEQ_DEV
    pairs_total = EXPERTS // TOPK
    pairs_group = GROUP_SIZE // TOPK
    hottest = jax.random.randint(key_hot, (), 0, EXPERTS)
    hot_group = hottest // GROUP_SIZE
    hot_inner = hottest % GROUP_SIZE
    perm_keys = jax.random.split(key_perm, blocks * GROUPS)
    perms = jax.vmap(lambda one_key: jax.random.permutation(one_key, GROUP_SIZE))(perm_keys)
    perms = perms.reshape(blocks, GROUPS, GROUP_SIZE)
    hot_perm = perms[:, hot_group, :]
    hot_place = jnp.argmax((hot_perm == hot_inner).astype(jnp.int32), axis=1)
    hot_pair = hot_group * pairs_group + hot_place // TOPK
    pair_keys = jax.random.split(key_pairs, blocks)
    order = jax.vmap(lambda one_key: jax.random.permutation(one_key, pairs_total))(pair_keys)
    hot_pos = jnp.argmax((order == hot_pair[:, None]).astype(jnp.int32), axis=1)
    starred = jax.random.randint(key_star, (blocks,), 0, SEQ_DEV)
    at_star = jnp.take_along_axis(order, starred[:, None], axis=1)[:, 0]
    places = jnp.arange(pairs_total)[None, :]
    order = jnp.where(places == starred[:, None], hot_pair[:, None], jnp.where(places == hot_pos[:, None], at_star[:, None], order))
    picked = order[:, :SEQ_DEV]
    groups = picked // pairs_group
    within = picked % pairs_group
    slot_index = within[:, :, None] * TOPK + jnp.arange(TOPK)[None, None, :]
    own_perm = perms[jnp.arange(blocks)[:, None], groups]
    inner = jnp.take_along_axis(own_perm, slot_index, axis=2)
    return (groups.reshape(TOKENS).astype(jnp.int32), inner.reshape(TOKENS, TOPK).astype(jnp.int32))


def draw_route_group(key, part):
    return routing_tables(key)[0]


def draw_route_inner(key, part):
    return routing_tables(key)[1]


def draw_lengths(key, part):
    base = jax.random.fold_in(key, 7101)
    key_len, key_top = jax.random.split(base, 2)
    spans = jax.random.randint(key_len, (TOKENS,), CACHE // 4, CACHE + 1)
    longest = jax.random.randint(key_top, (), 0, TOKENS)
    return jnp.where(jnp.arange(TOKENS) == longest, CACHE, spans).astype(jnp.int32)


def draw_head_bias(key, part):
    base = jax.random.fold_in(key, 7201)
    values = jax.random.uniform(base, (HEADS,), jnp.float32, -10.0, -4.0)
    return values


def draw_value_cache(key, part):
    base = jax.random.fold_in(key, 7301)
    key_common, key_noise = jax.random.split(base, 2)
    common = jax.random.normal(key_common, (TOKENS, KV_HEADS, 1, HEAD_SIZE), jnp.float32)
    noise = jax.random.normal(key_noise, (TOKENS, KV_HEADS, CACHE, HEAD_SIZE), jnp.float32)
    values = common + noise
    return jnp.clip(values, -7.0, 7.0).astype(jnp.bfloat16)


def levels(rng, dims, pieces, smallest, largest):
    level, own = 1.0, jax.random.fold_in(rng, 6)
    for position, parts in pieces:
        draws = jnp.exp(jax.random.uniform(jax.random.fold_in(own, position), (parts,), jnp.float32, smallest / len(pieces), largest / len(pieces)))
        level = level * jnp.repeat(draws, dims[position] // parts).reshape([-1 if axis == position else 1 for axis in range(len(dims))])
    return level


def centred(rng, dims, deviation, most, pieces=(), held_as=jnp.bfloat16):
    drawn = jax.random.normal(rng, dims, jnp.float32) * deviation
    if len(pieces) > 0:
        drawn = levels(rng, dims, pieces, -0.22, 0.18) * drawn
    return jnp.clip(drawn, min=-most, max=most).astype(held_as)


def setup_inputs(seed: int = 0) -> dict:
    streams_of = jax.random.split(jax.random.key(seed), 16)
    return {
        "hidden": centred(streams_of[0], (TOKENS, D), 1.0, 6.0, ((0, 128),)),
        "attn_gain": jnp.clip(jnp.exp(jax.random.uniform(streams_of[1], (D,), jnp.float32, math.log(0.3), math.log(3.0))), 0.3, 3.0),
        "query_weight": centred(streams_of[2], (D, HEADS * HEAD_SIZE), D ** -0.5, 0.125, ((0, 128), (1, 4))),
        "head_bias": draw_head_bias(jax.random.fold_in(streams_of[15], 71), 0),
        "key_cache": centred(streams_of[4], (TOKENS, KV_HEADS, CACHE, HEAD_SIZE), 1.0, 6.0, ((0, 128), (1, 4))),
        "value_cache": draw_value_cache(jax.random.fold_in(streams_of[15], 71), 0),
        "lengths": draw_lengths(jax.random.fold_in(streams_of[15], 71), 0),
        "out_weight": centred(streams_of[7], (HEADS * HEAD_SIZE, D), (HEADS * HEAD_SIZE) ** -0.5, 0.125, ((0, 4), (1, 128))),
        "moe_gain": jnp.clip(1.0 + 0.18 * jax.random.normal(streams_of[8], (D,), jnp.float32), 0.1, 1.9),
        "route_group": draw_route_group(jax.random.fold_in(streams_of[15], 71), 0),
        "route_inner": draw_route_inner(jax.random.fold_in(streams_of[15], 71), 0),
        "route_weight": jnp.clip(0.25 + 0.75 * jax.random.uniform(streams_of[11], (TOKENS, TOPK), jnp.float32) ** levels(streams_of[11], (TOKENS, TOPK), ((0, 128),), -0.2, 0.2), 0.25, 1.0).astype(jnp.bfloat16),
        "gate_w": centred(streams_of[12], (EXPERTS, D, FF_EXP), D ** -0.5, 0.125, ((0, 128), (2, 4))),
        "up_w": centred(streams_of[13], (EXPERTS, D, FF_EXP), D ** -0.5, 0.125, ((0, 128), (2, 4))),
        "down_w": centred(streams_of[14], (EXPERTS, FF_EXP, D), FF_EXP ** -0.5, 0.21875, ((0, 128), (1, 4))),
    }


rms_epsilon = 1e-06

def rms_scale(values, gain):
    wide = values.astype(jnp.float32)
    scaled = wide * lax.rsqrt(lax.optimization_barrier(jnp.mean(wide * wide, axis=-1, keepdims=True)) + rms_epsilon)
    return (scaled * gain).astype(jnp.bfloat16)

def attend(queries, key_cache, value_cache, lengths, head_bias):
    group_heads = HEADS // KV_HEADS
    bias_grid = head_bias.reshape(KV_HEADS, group_heads)

    def one_sequence(args):
        query_row, keys, values, length = args
        grouped = query_row.reshape(KV_HEADS, group_heads, HEAD_SIZE).astype(jnp.float32)
        scores = jnp.einsum('kgd,kpd->kgp', grouped, keys.astype(jnp.float32)) * HEAD_SIZE ** (-0.5)
        scores = scores + bias_grid[:, :, None]
        visible = jnp.arange(CACHE, dtype=jnp.int32) < length
        log_keep = jnp.where(visible[None, None, :], jax.nn.log_sigmoid(-scores), 0.0)
        later_sum = lax.cumsum(log_keep, axis=2, reverse=True) - log_keep
        weight = jnp.where(visible[None, None, :], jnp.exp(jax.nn.log_sigmoid(scores) + later_sum), 0.0)
        weight = weight.astype(jnp.bfloat16)
        result = jnp.einsum('kgp,kpd->kgd', weight.astype(jnp.float32), values.astype(jnp.float32))
        return result.astype(jnp.bfloat16).reshape(HEADS, HEAD_SIZE)
    return lax.map(one_sequence, (queries, key_cache, value_cache, lengths))

def reference(hidden, attn_gain, query_weight, head_bias, key_cache, value_cache, lengths, out_weight, moe_gain, route_group, route_inner, route_weight, gate_w, up_w, down_w):
    normed = rms_scale(hidden, attn_gain)
    queries = jnp.dot(normed, query_weight, preferred_element_type=jnp.float32).astype(jnp.bfloat16)
    queries = queries.reshape(TOKENS, HEADS, HEAD_SIZE)
    heads_out = attend(queries, key_cache, value_cache, lengths, head_bias).reshape(TOKENS, HEADS * HEAD_SIZE)
    head_width = HEADS * HEAD_SIZE // N_TP
    attended = jnp.zeros((TOKENS, D), jnp.float32)
    for group in range(N_TP):
        partial_value = jnp.dot(heads_out[:, group * head_width:(group + 1) * head_width], out_weight[group * head_width:(group + 1) * head_width], preferred_element_type=jnp.float32)
        attended = attended + lax.optimization_barrier(partial_value.astype(jnp.bfloat16)).astype(jnp.float32)
    residual = (hidden.astype(jnp.float32) + attended).astype(jnp.bfloat16)
    normed_two = rms_scale(residual, moe_gain)
    assigned = TOKENS * TOPK
    chosen = (route_group[:, None] * GROUP_SIZE + route_inner).reshape(assigned).astype(jnp.int32)
    padded_rows = jnp.concatenate([normed_two, jnp.zeros((1, D), jnp.bfloat16)], axis=0)
    weights_flat = jnp.concatenate([route_weight.reshape(assigned).astype(jnp.float32), jnp.zeros((1,), jnp.float32)], axis=0)
    ff_width = FF_EXP // N_TP

    def one_expert(expert):
        slots = jnp.nonzero(chosen == expert, size=N_EP, fill_value=assigned)[0].astype(jnp.int32)
        rows = padded_rows[slots // TOPK]
        gate_all = gate_w[expert]
        up_all = up_w[expert]
        down_all = down_w[expert]
        total = jnp.zeros((N_EP, D), jnp.float32)
        for group in range(N_TP):
            gated = jnp.dot(rows, gate_all[:, group * ff_width:(group + 1) * ff_width], preferred_element_type=jnp.float32)
            upped = jnp.dot(rows, up_all[:, group * ff_width:(group + 1) * ff_width], preferred_element_type=jnp.float32)
            activated = (jax.nn.silu(gated) * upped).astype(jnp.bfloat16)
            down_part = jnp.dot(activated, down_all[group * ff_width:(group + 1) * ff_width], preferred_element_type=jnp.float32)
            total = total + lax.optimization_barrier(down_part.astype(jnp.bfloat16)).astype(jnp.float32)
        return (slots, total.astype(jnp.bfloat16))
    slots, outputs = lax.map(one_expert, jnp.arange(EXPERTS, dtype=jnp.int32))
    contrib = weights_flat[slots][:, :, None] * outputs.astype(jnp.float32)
    collected = jnp.zeros((assigned + 1, D), jnp.float32).at[slots.reshape(-1)].add(contrib.reshape(-1, D))
    routed = lax.optimization_barrier(jnp.sum(collected[:assigned].reshape(TOKENS, TOPK, D), axis=1))
    return (residual.astype(jnp.float32) + routed).astype(jnp.bfloat16)
```

```python
import jax
import jax.numpy as jnp
from jax import lax
from jax.experimental import pallas as pl
from jax.experimental.pallas import tpu as pltpu
from jax.sharding import Mesh
from jax.sharding import PartitionSpec as P

EP = ("ep_0", "ep_1", "ep_2")
MESH = pl.DeviceIdType.MESH
F32 = jnp.float32
BF16 = jnp.bfloat16
NZ, NX, NC, NY = 16, 4, 2, 4
NXC = NX * NC
NSHORT = NXC * NY
EPS = 1e-06

NT = (((1,), (1,)), ((), ()))
TN = (((0,), (0,)), ((), ()))


def dot(a, b, dims=None, precision=None):
    if dims is None:
        dims = (((1,), (0,)), ((), ()))
    return lax.dot_general(a, b, dims, precision=precision, preferred_element_type=F32)


def iota(shape, dim):
    return lax.broadcasted_iota(jnp.int32, shape, dim)


def kernel(
    hid_ref,
    again_ref,
    wq_ref,
    bias_ref,
    k_hbm,
    v_hbm,
    len_ref,
    wo_ref,
    mgain_ref,
    rg_ref,
    ri_ref,
    rw_ref,
    gate_hbm,
    up_hbm,
    down_hbm,
    out_ref,
    k_v,
    v_v,
    wg_v,
    wu_v,
    wd_v,
    wq_g,
    wo_g,
    wo_t,
    sn,
    sh,
    sr,
    rn,
    rh,
    rr,
    sq,
    rq,
    so,
    ro,
    sp,
    rp,
    sd,
    rd,
    sx,
    rx,
    se,
    re,
    sf,
    rf,
    rres,
    load_sem,
    send_sem,
    recv_sem,
):
    z = lax.axis_index("ep_0")
    x = lax.axis_index("ep_1")
    c = lax.axis_index("ep_2")
    y = lax.axis_index("tp")
    xc = x * NC + c
    me = xc * NY + y

    loads = [
        pltpu.make_async_copy(k_hbm, k_v, load_sem.at[0]),
        pltpu.make_async_copy(v_hbm, v_v, load_sem.at[1]),
        pltpu.make_async_copy(down_hbm, wd_v, load_sem.at[2]),
    ]
    for half in range(2):
        loads.append(pltpu.make_async_copy(gate_hbm.at[:, half], wg_v.at[half], load_sem.at[3 + half]))
        loads.append(pltpu.make_async_copy(up_hbm.at[:, half], wu_v.at[half], load_sem.at[5 + half]))
    for one in loads:
        one.start()

    def z_of(i):
        off = (i + 1) // 2
        return (z + 8 + jnp.where(i % 2 == 1, NZ - off, off)) % NZ

    def short_of(j):
        p = (me + j) % NSHORT
        return p // NY, p % NY

    barrier = pltpu.get_barrier_semaphore()

    def greet_z(i, carry):
        pl.semaphore_signal(barrier, inc=1, device_id={"ep_0": z_of(i)}, device_id_type=MESH)
        return carry

    def greet_short(j, carry):
        pxc, py = short_of(j)
        pl.semaphore_signal(
            barrier, inc=1, device_id={"ep_1": pxc // NC, "ep_2": pxc % NC, "tp": py}, device_id_type=MESH
        )
        return carry

    lax.fori_loop(0, NZ - 1, greet_z, 0)
    lax.fori_loop(1, NSHORT, greet_short, 0)

    hid = hid_ref[...].astype(F32)
    scale = lax.rsqrt(jnp.mean(hid * hid, axis=-1, keepdims=True) + EPS)
    hid2 = jnp.concatenate([hid, hid], axis=0)
    scale2 = jnp.concatenate([scale, scale], axis=0)
    for k in range(NZ):
        part = hid2[:, 128 * k : 128 * k + 128]
        sn[k] = (part * scale2 * again_ref[k : k + 1, :]).astype(BF16)
        sh[k] = part.astype(BF16)

    eye = (iota((16, 16), 0) == iota((16, 16), 1)).astype(BF16)
    wo_t[...] = dot(eye, wo_ref[...], NT).astype(BF16)

    lane = iota((1, 128), 1)
    tok_a = lane % 4
    near = (lane // 4) == z
    wide = (lane // 8) == z
    route_w = rw_ref[...].astype(F32)
    rows = []
    for pattern in (near, wide):
        for k in range(2):
            row = jnp.zeros((1, 128), F32)
            for t in range(4):
                ident = (rg_ref[t] * 32 + ri_ref[2 * t + k]).astype(F32)
                row = jnp.where(tok_a == t, ident, row)
            rows.append(jnp.where(pattern, row, 0.0))
    for k in range(2):
        spread = jnp.where(
            (iota((4, 128), 1) % 4) == iota((4, 128), 0), jnp.broadcast_to(route_w[:, k : k + 1], (4, 128)), 0.0
        )
        rows.append(jnp.where(wide, jnp.sum(spread, axis=0, keepdims=True), 0.0))
    rowid = iota((8, 128), 0)
    packet = jnp.zeros((8, 128), F32)
    for k, row in enumerate(rows):
        packet = jnp.where(rowid == k, jnp.broadcast_to(row, (8, 128)), packet)
    sr[...] = packet.astype(BF16)

    pl.semaphore_wait(barrier, NZ - 1 + NSHORT - 1)

    def to_z(i, src, dst, phase):
        return pltpu.make_async_remote_copy(
            src_ref=src,
            dst_ref=dst,
            send_sem=send_sem.at[phase],
            recv_sem=recv_sem.at[phase],
            device_id={"ep_0": z_of(i)},
            device_id_type=MESH,
        )

    def to_short(pxc, py, src, dst, phase):
        return pltpu.make_async_remote_copy(
            src_ref=src,
            dst_ref=dst,
            send_sem=send_sem.at[phase],
            recv_sem=recv_sem.at[phase],
            device_id={"ep_1": pxc // NC, "ep_2": pxc % NC, "tp": py},
            device_id_type=MESH,
        )

    def all_of(ref, phase):
        return pltpu.make_async_remote_copy(
            src_ref=ref,
            dst_ref=ref,
            send_sem=send_sem.at[phase],
            recv_sem=recv_sem.at[phase],
            device_id={"ep_0": (z + 1) % NZ},
            device_id_type=MESH,
        )

    def z_exchange(src_of, dst, phase):
        def go(i, carry):
            to_z(i, src_of(z_of(i)), dst, phase).start()
            return carry

        lax.fori_loop(0, NZ - 1, go, 0)

    z_exchange(lambda p: sn.at[p], rn.at[z], 0)

    def gather_weights(src, dst, phase):
        def go(j, carry):
            p = (xc + j) % NXC
            to_short(p, y, src, dst.at[xc], phase).start()
            return carry

        lax.fori_loop(1, NXC, go, 0)

    gather_weights(wq_ref, wq_g, 1)
    z_exchange(lambda p: sr, rr.at[z], 3)
    z_exchange(lambda p: sh.at[p], rh.at[z], 2)
    gather_weights(wo_t, wo_g, 4)
    rn[z] = sn[z]
    rr[z] = sr[...]
    rh[z] = sh[z]
    wq_g[xc] = wq_ref[...]
    wo_g[xc] = wo_t[...]

    all_of(rn.at[0 : NZ - 1], 0).wait_recv()
    all_of(wq_g.at[0 : NXC - 1], 1).wait_recv()

    first = (iota((128, 128), 0) % 8) < 4
    xin = rn[...].astype(F32).reshape(128, 128).astype(BF16)
    wq_z = wq_g[...].reshape(128, 512)
    part_q = dot(xin, wq_z)
    for p in range(2):
        pair = jnp.where(first, part_q[:, 256 * p : 256 * p + 128], part_q[:, 256 * p + 128 : 256 * p + 256])
        sq[:, p] = pair.reshape(NZ, 8, 128).astype(BF16)
    z_exchange(lambda p: sq.at[p], rq.at[z], 5)
    rq[z] = sq[z]

    later = (iota((128, 128), 0) > iota((128, 128), 1)).astype(F32)
    rowh = iota((16, 1), 0)
    bias = jnp.zeros((16, 1), F32)
    length = jnp.zeros((16, 1), jnp.int32)
    for h in range(4):
        bias = jnp.where(rowh // 4 == h, bias_ref[4 * y + h], bias)
        length = jnp.where(rowh % 4 == h, len_ref[h], length)

    all_of(rq.at[0 : NZ - 1], 5).wait_recv()
    q = jnp.sum(rq[...].astype(F32), axis=0).reshape(16, 128).astype(BF16)
    loads[0].wait()
    tok = iota((16, 1024), 0) % 4
    scores = jnp.zeros((16, 1024), F32)
    for t in range(4):
        scores = jnp.where(tok == t, dot(q, k_v[t], NT), scores)
    scores = scores * (128.0 ** -0.5) + bias
    soft = jnp.log1p(jnp.exp(-jnp.abs(scores)))
    log_stop = jnp.minimum(scores, 0.0) - soft
    visible = iota((16, 1024), 1) < length
    log_keep = jnp.where(visible, log_stop - scores, 0.0)
    stacked = jnp.concatenate([log_keep[:, 128 * k : 128 * k + 128] for k in range(8)], axis=0)
    within = dot(stacked, later, precision=lax.Precision.HIGHEST)
    carry_sum = jnp.zeros((16, 1), F32)
    weights = [None] * 8
    for k in reversed(range(8)):
        inner = within[16 * k : 16 * k + 16]
        keep_k = log_keep[:, 128 * k : 128 * k + 128]
        expo = jnp.exp(log_stop[:, 128 * k : 128 * k + 128] + (inner + carry_sum))
        weights[k] = jnp.where(visible[:, 128 * k : 128 * k + 128], expo, 0.0)
        carry_sum = carry_sum + (inner[:, 0:1] + keep_k[:, 0:1])
    weight = jnp.concatenate(weights, axis=1).astype(BF16)
    loads[1].wait()
    tok_o = iota((16, 128), 0) % 4
    heads = jnp.zeros((16, 128), F32)
    for t in range(4):
        heads = jnp.where(tok_o == t, dot(weight, v_v[t]), heads)
    so[...] = heads.astype(BF16)

    z_exchange(lambda p: so, ro.at[z], 6)
    ro[z] = so[...]
    all_of(wo_g.at[0 : NXC - 1], 4).wait_recv()
    wo_z = wo_g[...].reshape(128, 512)
    head_row = (iota((256, 128), 0) % 16) // 4
    all_of(ro.at[0 : NZ - 1], 6).wait_recv()
    heads_in = ro[...].reshape(256, 128)
    proj = jnp.zeros((256, 128), F32)
    for h in range(4):
        proj = jnp.where(head_row == h, dot(heads_in, wo_z[:, 128 * h : 128 * h + 128], NT), proj)
    proj = jnp.sum(proj.reshape(NZ, 2, 8, 128), axis=1)
    proj = proj + pltpu.roll(proj, 4, 1)
    sp[...] = proj.reshape(4, 4, 8, 128).astype(BF16)

    def send_part(j, carry):
        py = (y + j) % NY
        to_short(xc, py, sp.at[py], rp.at[y], 7).start()
        return carry

    lax.fori_loop(1, NY, send_part, 0)
    rp[y] = sp[y]

    all_of(rr.at[0 : NZ - 1], 3).wait_recv()
    route = jnp.sum(rr[...].astype(F32), axis=0)
    mine = pltpu.roll(route, (128 - 16 * y) % 128, 1)
    slot_row = iota((64, 16), 0)
    slot_expert = (NXC * z + slot_row // 8).astype(F32)
    same_block = (slot_row % 4) == (iota((64, 16), 1) // 4)
    wanted = (mine[0:1, 0:16] == slot_expert) | (mine[1:2, 0:16] == slot_expert)
    select = jnp.where(same_block & wanted, 1.0, 0.0).astype(BF16)

    all_of(rh.at[0 : NZ - 1], 2).wait_recv()
    own_hidden = rh[pl.ds(4 * y, 4)].astype(F32)
    all_of(rp.at[0 : NY - 1], 7).wait_recv()
    resid = own_hidden + jnp.sum(rp[...].astype(F32), axis=0)
    first8 = iota((8, 128), 0) < 4
    sd[...] = jnp.concatenate(
        [jnp.where(first8, resid[0], resid[1]), jnp.where(first8, resid[2], resid[3])], axis=0
    ).astype(BF16)

    z_exchange(lambda p: sd, rd.at[z], 8)
    rd[z] = sd[...]

    crow = iota((256, 128), 0)
    clane = iota((256, 128), 1)
    cexp = (NXC * z + crow // 32).astype(F32)
    cblock = (crow // 8) % 4 * 4 + crow % 4
    cmatch = (cblock == clane // 8) & (((crow // 4) % 2) == ((clane // 4) % 2))
    cweight = jnp.where(route[2:3] == cexp, route[4:5], 0.0) + jnp.where(route[3:4] == cexp, route[5:6], 0.0)
    combine = jnp.where(cmatch, cweight, 0.0).astype(BF16)

    all_of(rd.at[0 : NZ - 1], 8).wait_recv()
    rows_in = rd[...].astype(F32)
    square = jnp.sum(jnp.sum(rows_in * rows_in, axis=0), axis=-1, keepdims=True) * (1.0 / 2048.0)
    scale_two = lax.rsqrt(square + EPS)
    normed = jnp.concatenate(
        [(rows_in[k] * scale_two * mgain_ref[k : k + 1, :]).astype(BF16) for k in range(NZ)], axis=1
    )
    slots = dot(select, normed)
    first64 = (iota((64, 128), 0) % 8) < 4
    for m in range(8):
        pair = jnp.where(first64, slots[:, 256 * m : 256 * m + 128], slots[:, 256 * m + 128 : 256 * m + 256])
        sx[:, m] = pair.reshape(NXC, 8, 128).astype(BF16)

    def send_slots(j, carry):
        pxc, py = short_of(j)
        to_short(pxc, py, sx.at[pxc], rx.at[me], 9).start()
        return carry

    lax.fori_loop(1, NSHORT, send_slots, 0)
    rx[me] = sx[xc]

    owner = z // 4

    @pl.when(y == owner)
    def _():
        def send_rows(j, carry):
            py = (y + j) % NY
            to_short(xc, py, rd.at[pl.ds(4 * py, 4)], rres, 12).start()
            return carry

        lax.fori_loop(1, NY, send_rows, 0)
        rres[...] = rd[pl.ds(4 * y, 4)]

    for one in loads[2:]:
        one.wait()
    all_of(rx.at[0 : NSHORT - 1], 9).wait_recv()
    lhs = jnp.concatenate([rx[:, m].astype(F32).reshape(256, 128).astype(BF16) for m in range(8)], axis=1)
    first_ff = (iota((256, 192), 0) % 8) < 4

    def swap(v):
        return pltpu.roll(v.reshape(32, 8, 192), 4, 1).reshape(256, 192)

    def both_halves(w):
        both = jnp.where(first_ff, dot(lhs, w[0].reshape(1024, 192)), dot(lhs, w[1].reshape(1024, 192)))
        return both + swap(both)

    gated = both_halves(wg_v)
    upped = both_halves(wu_v)
    act = (gated / (1.0 + jnp.exp(-gated)) * upped).astype(BF16)

    first256 = (iota((256, 128), 0) % 8) < 4
    for m in range(8):
        down_a = dot(act, wd_v[:, 256 * m : 256 * m + 128])
        down_b = dot(act, wd_v[:, 256 * m + 128 : 256 * m + 256])
        pair = jnp.where(first256, down_a, down_b).reshape(NXC, NY, 8, 128).astype(BF16)
        se[:, m // 2, m % 2] = pair

    def send_back(j, carry):
        pxc, py = short_of(j)
        to_short(pxc, py, se.at[pxc, py], re.at[me], 10).start()
        return carry

    lax.fori_loop(1, NSHORT, send_back, 0)
    re[me] = se[xc, y]

    all_of(re.at[0 : NSHORT - 1], 10).wait_recv()
    for m in range(2):
        total = jnp.sum(re[:, m].astype(F32).reshape(NXC, NY, NY * 8, 128), axis=1)
        total = total.reshape(256, 128).astype(BF16)
        mixed = dot(combine, total, TN)
        sf[:, m] = mixed.reshape(NZ, 8, 128).astype(BF16)

    z_exchange(lambda p: sf.at[p], rf.at[z], 11)
    rf[z] = sf[z]

    @pl.when(y != owner)
    def _():
        all_of(rres, 12).wait_recv()

    pick = (iota((4, 16), 1) == 4 * (z % 4) + iota((4, 16), 0)).astype(BF16)
    own_rows = [dot(pick, rres[k]) for k in range(4)]
    all_of(rf.at[0 : NZ - 1], 11).wait_recv()
    routed = jnp.sum(rf[...].astype(F32), axis=0).reshape(16, 128)
    for k in range(4):
        out_ref[:, 128 * k : 128 * k + 128] = (own_rows[k] + routed[4 * k : 4 * k + 4]).astype(BF16)

    for ref, phase in (
        (rn.at[0 : NZ - 1], 0),
        (wq_g.at[0 : NXC - 1], 1),
        (rh.at[0 : NZ - 1], 2),
        (rr.at[0 : NZ - 1], 3),
        (wo_g.at[0 : NXC - 1], 4),
        (rq.at[0 : NZ - 1], 5),
        (ro.at[0 : NZ - 1], 6),
        (rp.at[0 : NY - 1], 7),
        (rd.at[0 : NZ - 1], 8),
        (rx.at[0 : NSHORT - 1], 9),
        (re.at[0 : NSHORT - 1], 10),
        (rf.at[0 : NZ - 1], 11),
    ):
        all_of(ref, phase).wait_send()

    @pl.when(y == owner)
    def _():
        all_of(rd.at[0:12], 12).wait_send()


def body(
    hidden,
    attn_gain,
    query_weight,
    head_bias,
    key_cache,
    value_cache,
    lengths,
    out_weight,
    moe_gain,
    route_group,
    route_inner,
    route_weight,
    gate_w,
    up_w,
    down_w,
):
    vmem = pl.BlockSpec(memory_space=pltpu.VMEM)
    smem = pl.BlockSpec(memory_space=pltpu.SMEM)
    hbm = pl.BlockSpec(memory_space=pl.ANY)

    def buf(*shape):
        return pltpu.VMEM(shape, BF16)

    return pl.pallas_call(
        kernel,
        out_shape=jax.ShapeDtypeStruct((4, 512), BF16),
        in_specs=[vmem, vmem, vmem, smem, hbm, hbm, smem, vmem, vmem, smem, smem, vmem, hbm, hbm, hbm],
        out_specs=vmem,
        scratch_shapes=[
            buf(4, 1024, 128),
            buf(4, 1024, 128),
            buf(2, 8, 128, 192),
            buf(2, 8, 128, 192),
            buf(192, 2048),
            buf(NXC, 16, 512),
            buf(NXC, 16, 512),
            buf(16, 512),
            buf(NZ, 8, 128),
            buf(NZ, 8, 128),
            buf(8, 128),
            buf(NZ, 8, 128),
            buf(NZ, 8, 128),
            buf(NZ, 8, 128),
            buf(NZ, 2, 8, 128),
            buf(NZ, 2, 8, 128),
            buf(16, 128),
            buf(NZ, 16, 128),
            buf(NY, 4, 8, 128),
            buf(NY, 4, 8, 128),
            buf(16, 128),
            buf(NZ, 16, 128),
            buf(NXC, 8, 8, 128),
            buf(NSHORT, 8, 8, 128),
            buf(NXC, NY, 2, NY, 8, 128),
            buf(NSHORT, 2, NY, 8, 128),
            buf(NZ, 2, 8, 128),
            buf(NZ, 2, 8, 128),
            buf(4, 16, 128),
            pltpu.SemaphoreType.DMA((7,)),
            pltpu.SemaphoreType.DMA((13,)),
            pltpu.SemaphoreType.DMA((13,)),
        ],
        compiler_params=pltpu.CompilerParams(
            collective_id=0, has_side_effects=True, vmem_limit_bytes=40 * 1024 * 1024
        ),
        name="layer",
    )(
        hidden,
        attn_gain.reshape(16, 128),
        query_weight,
        head_bias,
        key_cache.reshape(4, 1024, 128),
        value_cache.reshape(4, 1024, 128),
        lengths,
        out_weight,
        moe_gain.reshape(16, 128),
        route_group,
        route_inner.reshape(8),
        route_weight,
        gate_w.reshape(8, 2, 128, 192),
        up_w.reshape(8, 2, 128, 192),
        down_w.reshape(192, 2048),
    )


def solution(mesh):
    torus = Mesh(mesh.devices.reshape(NZ, NX, NC, NY), ("ep_0", "ep_1", "ep_2", "tp"))
    placed = (
        P(EP, None),
        P(),
        P(EP, "tp"),
        P(),
        P(EP, "tp", None, None),
        P(EP, "tp", None, None),
        P(EP),
        P("tp", EP),
        P(),
        P(EP),
        P(EP, None),
        P(EP, None),
        P(EP, None, "tp"),
        P(EP, None, "tp"),
        P(EP, "tp", None),
    )
    return jax.shard_map(body, mesh=torus, in_specs=placed, out_specs=P(EP, "tp"), check_vma=False)
```

```python
import jax
import jax.numpy as jnp
from jax import lax
from jax.experimental import pallas as pl
from jax.experimental.pallas import tpu as pltpu
from jax.sharding import Mesh
from jax.sharding import PartitionSpec as P

EP = ("ep_0", "ep_1", "ep_2")
MESH = pl.DeviceIdType.MESH
F32 = jnp.float32
BF16 = jnp.bfloat16
NZ, NX, NC, NY = 16, 4, 2, 4
NXC = NX * NC
NSHORT = NXC * NY
EPS = 1e-06

NT = (((1,), (1,)), ((), ()))
TN = (((0,), (0,)), ((), ()))


def dot(a, b, dims=None, precision=None):
    if dims is None:
        dims = (((1,), (0,)), ((), ()))
    return lax.dot_general(a, b, dims, precision=precision, preferred_element_type=F32)


def iota(shape, dim):
    return lax.broadcasted_iota(jnp.int32, shape, dim)


def kernel(
    hid_hbm,
    again_hbm,
    wq_hbm,
    bias_hbm,
    k_hbm,
    v_hbm,
    len_hbm,
    wo_hbm,
    mgain_hbm,
    rg_hbm,
    ri_hbm,
    rw_hbm,
    gate_hbm,
    up_hbm,
    down_hbm,
    out_ref,
    hid_ref,
    again_ref,
    wq_ref,
    bias_ref,
    len_ref,
    wo_t,
    mgain_ref,
    rg_ref,
    ri_ref,
    rw_ref,
    k_v,
    v_v,
    wg_v,
    wu_v,
    wd_v,
    wq_g,
    wo_g,
    sn,
    sh,
    sr,
    rn,
    rh,
    rr,
    sq,
    rq,
    so,
    ro,
    sp,
    rp,
    sd,
    rd,
    sx,
    rx,
    se,
    re,
    sf,
    rf,
    rres,
    load_sem,
    send_sem,
    recv_sem,
):
    z = lax.axis_index("ep_0")
    x = lax.axis_index("ep_1")
    c = lax.axis_index("ep_2")
    y = lax.axis_index("tp")
    xc = x * NC + c
    me = xc * NY + y

    def z_of(i):
        off = (i + 1) // 2
        return (z + 8 + jnp.where(i % 2 == 1, NZ - off, off)) % NZ

    def short_of(j):
        p = (me + j) % NSHORT
        return p // NY, p % NY

    barrier = pltpu.get_barrier_semaphore()

    def greet_z(i, carry):
        pl.semaphore_signal(barrier, inc=1, device_id={"ep_0": z_of(i)}, device_id_type=MESH)
        return carry

    def greet_short(j, carry):
        pxc, py = short_of(j)
        pl.semaphore_signal(
            barrier, inc=1, device_id={"ep_1": pxc // NC, "ep_2": pxc % NC, "tp": py}, device_id_type=MESH
        )
        return carry

    lax.fori_loop(0, NZ - 1, greet_z, 0)
    lax.fori_loop(1, NSHORT, greet_short, 0)

    copies = (
        (hid_hbm, hid_ref),
        (again_hbm, again_ref),
        (rw_hbm, rw_ref),
        (rg_hbm, rg_ref),
        (ri_hbm, ri_ref),
        (wq_hbm, wq_ref),
        (wo_hbm, wo_t),
        (bias_hbm, bias_ref),
        (len_hbm, len_ref),
        (mgain_hbm, mgain_ref),
        (k_hbm, k_v),
        (v_hbm, v_v),
        (gate_hbm, wg_v),
        (up_hbm, wu_v),
        (down_hbm, wd_v),
    )
    loads = [pltpu.make_async_copy(src, dst, load_sem.at[i]) for i, (src, dst) in enumerate(copies)]
    for one in loads:
        one.start()
    for one in loads[0:5]:
        one.wait()

    hid = hid_ref[...].astype(F32)
    scale = lax.rsqrt(jnp.mean(hid * hid, axis=-1, keepdims=True) + EPS)
    hid2 = jnp.concatenate([hid, hid], axis=0)
    scale2 = jnp.concatenate([scale, scale], axis=0)
    for k in range(NZ):
        part = hid2[:, 128 * k : 128 * k + 128]
        sn[k] = (part * scale2 * again_ref[k : k + 1, :]).astype(BF16)
        sh[k] = part.astype(BF16)

    lane = iota((1, 128), 1)
    tok_a = lane % 4
    near = (lane // 4) == z
    wide = (lane // 8) == z
    route_w = rw_ref[...].astype(F32)
    rows = []
    for pattern in (near, wide):
        for k in range(2):
            row = jnp.zeros((1, 128), F32)
            for t in range(4):
                ident = (rg_ref[t] * 32 + ri_ref[k, t]).astype(F32)
                row = jnp.where(tok_a == t, ident, row)
            rows.append(jnp.where(pattern, row, 0.0))
    for k in range(2):
        row = jnp.zeros((1, 128), F32)
        for t in range(4):
            row = jnp.where(tok_a == t, route_w[k : k + 1, t : t + 1], row)
        rows.append(jnp.where(wide, row, 0.0))
    rowid = iota((8, 128), 0)
    packet = jnp.zeros((8, 128), F32)
    for k, row in enumerate(rows):
        packet = jnp.where(rowid == k, jnp.broadcast_to(row, (8, 128)), packet)
    sr[...] = packet.astype(BF16)

    for one in loads[5:10]:
        one.wait()
    pl.semaphore_wait(barrier, NZ - 1 + NSHORT - 1)

    def to_z(i, src, dst, phase):
        return pltpu.make_async_remote_copy(
            src_ref=src,
            dst_ref=dst,
            send_sem=send_sem.at[phase],
            recv_sem=recv_sem.at[phase],
            device_id={"ep_0": z_of(i)},
            device_id_type=MESH,
        )

    def to_short(pxc, py, src, dst, phase):
        return pltpu.make_async_remote_copy(
            src_ref=src,
            dst_ref=dst,
            send_sem=send_sem.at[phase],
            recv_sem=recv_sem.at[phase],
            device_id={"ep_1": pxc // NC, "ep_2": pxc % NC, "tp": py},
            device_id_type=MESH,
        )

    def all_of(ref, phase):
        return pltpu.make_async_remote_copy(
            src_ref=ref,
            dst_ref=ref,
            send_sem=send_sem.at[phase],
            recv_sem=recv_sem.at[phase],
            device_id={"ep_0": (z + 1) % NZ},
            device_id_type=MESH,
        )

    def z_exchange(src_of, dst, phase):
        def go(i, carry):
            to_z(i, src_of(z_of(i)), dst, phase).start()
            return carry

        lax.fori_loop(0, NZ - 1, go, 0)

    z_exchange(lambda p: sn.at[p], rn.at[z], 0)

    def gather_weights(src, dst, phase):
        def go(j, carry):
            p = (xc + j) % NXC
            to_short(p, y, src, dst.at[xc], phase).start()
            return carry

        lax.fori_loop(1, NXC, go, 0)

    gather_weights(wq_ref, wq_g, 1)
    z_exchange(lambda p: sr, rr.at[z], 3)
    z_exchange(lambda p: sh.at[p], rh.at[z], 2)
    gather_weights(wo_t, wo_g, 4)
    rn[z] = sn[z]
    rr[z] = sr[...]
    rh[z] = sh[z]
    wq_g[xc] = wq_ref[...]
    wo_g[xc] = wo_t[...]

    all_of(rn.at[0 : NZ - 1], 0).wait_recv()
    all_of(wq_g.at[0 : NXC - 1], 1).wait_recv()

    first = (iota((128, 128), 0) % 8) < 4
    xin = rn[...].astype(F32).reshape(128, 128).astype(BF16)
    wq_z = wq_g[...].reshape(128, 512)
    part_q = dot(xin, wq_z)
    for p in range(2):
        pair = jnp.where(first, part_q[:, 256 * p : 256 * p + 128], part_q[:, 256 * p + 128 : 256 * p + 256])
        sq[:, p] = pair.reshape(NZ, 8, 128).astype(BF16)
    z_exchange(lambda p: sq.at[p], rq.at[z], 5)
    rq[z] = sq[z]

    later = (iota((128, 128), 0) > iota((128, 128), 1)).astype(F32)
    rowh = iota((16, 1), 0)
    bias = jnp.zeros((16, 1), F32)
    length = jnp.zeros((16, 1), jnp.int32)
    for h in range(4):
        bias = jnp.where(rowh // 4 == h, bias_ref[4 * y + h], bias)
        length = jnp.where(rowh % 4 == h, len_ref[h], length)

    all_of(rq.at[0 : NZ - 1], 5).wait_recv()
    q = jnp.sum(rq[...].astype(F32), axis=0).reshape(16, 128).astype(BF16)
    loads[10].wait()
    tok = iota((16, 1024), 0) % 4
    scores = jnp.zeros((16, 1024), F32)
    for t in range(4):
        scores = jnp.where(tok == t, dot(q, k_v[t], NT), scores)
    scores = scores * (128.0 ** -0.5) + bias
    soft = jnp.log1p(jnp.exp(-jnp.abs(scores)))
    log_stop = jnp.minimum(scores, 0.0) - soft
    visible = iota((16, 1024), 1) < length
    log_keep = jnp.where(visible, log_stop - scores, 0.0)
    stacked = jnp.concatenate([log_keep[:, 128 * k : 128 * k + 128] for k in range(8)], axis=0)
    within = dot(stacked, later, precision=lax.Precision.HIGHEST)
    carry_sum = jnp.zeros((16, 1), F32)
    weights = [None] * 8
    for k in reversed(range(8)):
        inner = within[16 * k : 16 * k + 16]
        keep_k = log_keep[:, 128 * k : 128 * k + 128]
        expo = jnp.exp(log_stop[:, 128 * k : 128 * k + 128] + (inner + carry_sum))
        weights[k] = jnp.where(visible[:, 128 * k : 128 * k + 128], expo, 0.0)
        carry_sum = carry_sum + (inner[:, 0:1] + keep_k[:, 0:1])
    weight = jnp.concatenate(weights, axis=1).astype(BF16)
    loads[11].wait()
    tok_o = iota((16, 128), 0) % 4
    heads = jnp.zeros((16, 128), F32)
    for t in range(4):
        heads = jnp.where(tok_o == t, dot(weight, v_v[t]), heads)
    so[...] = heads.astype(BF16)

    z_exchange(lambda p: so, ro.at[z], 6)
    ro[z] = so[...]
    all_of(wo_g.at[0 : NXC - 1], 4).wait_recv()
    wo_z = wo_g[...].reshape(128, 512)
    head_row = (iota((256, 128), 0) % 16) // 4
    all_of(ro.at[0 : NZ - 1], 6).wait_recv()
    heads_in = ro[...].reshape(256, 128)
    proj = jnp.zeros((256, 128), F32)
    for h in range(4):
        proj = jnp.where(head_row == h, dot(heads_in, wo_z[:, 128 * h : 128 * h + 128], NT), proj)
    proj = jnp.sum(proj.reshape(NZ, 2, 8, 128), axis=1)
    proj = proj + pltpu.roll(proj, 4, 1)
    sp[...] = proj.reshape(4, 4, 8, 128).astype(BF16)

    def send_part(j, carry):
        py = (y + j) % NY
        to_short(xc, py, sp.at[py], rp.at[y], 7).start()
        return carry

    lax.fori_loop(1, NY, send_part, 0)
    rp[y] = sp[y]

    all_of(rr.at[0 : NZ - 1], 3).wait_recv()
    route = jnp.sum(rr[...].astype(F32), axis=0)
    mine = pltpu.roll(route, (128 - 16 * y) % 128, 1)
    slot_row = iota((64, 16), 0)
    slot_expert = (NXC * z + slot_row // 8).astype(F32)
    same_block = (slot_row % 4) == (iota((64, 16), 1) // 4)
    wanted = (mine[0:1, 0:16] == slot_expert) | (mine[1:2, 0:16] == slot_expert)
    select = jnp.where(same_block & wanted, 1.0, 0.0).astype(BF16)

    all_of(rh.at[0 : NZ - 1], 2).wait_recv()
    own_hidden = rh[pl.ds(4 * y, 4)].astype(F32)
    all_of(rp.at[0 : NY - 1], 7).wait_recv()
    resid = own_hidden + jnp.sum(rp[...].astype(F32), axis=0)
    first8 = iota((8, 128), 0) < 4
    sd[...] = jnp.concatenate(
        [jnp.where(first8, resid[0], resid[1]), jnp.where(first8, resid[2], resid[3])], axis=0
    ).astype(BF16)

    z_exchange(lambda p: sd, rd.at[z], 8)
    rd[z] = sd[...]

    crow = iota((256, 128), 0)
    clane = iota((256, 128), 1)
    cexp = (NXC * z + crow // 32).astype(F32)
    cblock = (crow // 8) % 4 * 4 + crow % 4
    cmatch = (cblock == clane // 8) & (((crow // 4) % 2) == ((clane // 4) % 2))
    cweight = jnp.where(route[2:3] == cexp, route[4:5], 0.0) + jnp.where(route[3:4] == cexp, route[5:6], 0.0)
    combine = jnp.where(cmatch, cweight, 0.0).astype(BF16)

    all_of(rd.at[0 : NZ - 1], 8).wait_recv()
    rows_in = rd[...].astype(F32)
    square = jnp.sum(jnp.sum(rows_in * rows_in, axis=0), axis=-1, keepdims=True) * (1.0 / 2048.0)
    scale_two = lax.rsqrt(square + EPS)
    normed = jnp.concatenate(
        [(rows_in[k] * scale_two * mgain_ref[k : k + 1, :]).astype(BF16) for k in range(NZ)], axis=1
    )
    slots = dot(select, normed)
    first64 = (iota((64, 128), 0) % 8) < 4
    for m in range(8):
        pair = jnp.where(first64, slots[:, 128 * m : 128 * m + 128], slots[:, 1024 + 128 * m : 1152 + 128 * m])
        sx[:, m] = pair.reshape(NXC, 8, 128).astype(BF16)

    def send_slots(j, carry):
        pxc, py = short_of(j)
        to_short(pxc, py, sx.at[pxc], rx.at[me], 9).start()
        return carry

    lax.fori_loop(1, NSHORT, send_slots, 0)
    rx[me] = sx[xc]

    owner = z // 4

    @pl.when(y == owner)
    def _():
        def send_rows(j, carry):
            py = (y + j) % NY
            to_short(xc, py, rd.at[pl.ds(4 * py, 4)], rres, 12).start()
            return carry

        lax.fori_loop(1, NY, send_rows, 0)
        rres[...] = rd[pl.ds(4 * y, 4)]

    for one in loads[12:]:
        one.wait()
    all_of(rx.at[0 : NSHORT - 1], 9).wait_recv()
    lhs = jnp.concatenate([rx[:, m].astype(F32).reshape(256, 128).astype(BF16) for m in range(8)], axis=1)
    first_ff = (iota((256, 192), 0) % 8) < 4

    def swap(v):
        return pltpu.roll(v.reshape(32, 8, 192), 4, 1).reshape(256, 192)

    def both_halves(w):
        both = jnp.where(first_ff, dot(lhs, w[:, 0:1024], NT), dot(lhs, w[:, 1024:2048], NT))
        return both + swap(both)

    gated = both_halves(wg_v)
    upped = both_halves(wu_v)
    act = (gated / (1.0 + jnp.exp(-gated)) * upped).astype(BF16)

    first256 = (iota((256, 128), 0) % 8) < 4
    for m in range(8):
        down_a = dot(act, wd_v[:, 256 * m : 256 * m + 128])
        down_b = dot(act, wd_v[:, 256 * m + 128 : 256 * m + 256])
        pair = jnp.where(first256, down_a, down_b).reshape(NXC, NY, 8, 128).astype(BF16)
        se[:, m // 2, m % 2] = pair

    def send_back(j, carry):
        pxc, py = short_of(j)
        to_short(pxc, py, se.at[pxc, py], re.at[me], 10).start()
        return carry

    lax.fori_loop(1, NSHORT, send_back, 0)
    re[me] = se[xc, y]

    all_of(re.at[0 : NSHORT - 1], 10).wait_recv()
    for m in range(2):
        total = jnp.sum(re[:, m].astype(F32).reshape(NXC, NY, NY * 8, 128), axis=1)
        total = total.reshape(256, 128).astype(BF16)
        mixed = dot(combine, total, TN)
        sf[:, m] = mixed.reshape(NZ, 8, 128).astype(BF16)

    z_exchange(lambda p: sf.at[p], rf.at[z], 11)
    rf[z] = sf[z]

    @pl.when(y != owner)
    def _():
        all_of(rres, 12).wait_recv()

    pick = (iota((4, 16), 1) == 4 * (z % 4) + iota((4, 16), 0)).astype(BF16)
    own_rows = [dot(pick, rres[k]) for k in range(4)]
    all_of(rf.at[0 : NZ - 1], 11).wait_recv()
    routed = jnp.sum(rf[...].astype(F32), axis=0).reshape(16, 128)
    for k in range(4):
        out_ref[:, 128 * k : 128 * k + 128] = (own_rows[k] + routed[4 * k : 4 * k + 4]).astype(BF16)

    for ref, phase in (
        (rn.at[0 : NZ - 1], 0),
        (wq_g.at[0 : NXC - 1], 1),
        (rh.at[0 : NZ - 1], 2),
        (rr.at[0 : NZ - 1], 3),
        (wo_g.at[0 : NXC - 1], 4),
        (rq.at[0 : NZ - 1], 5),
        (ro.at[0 : NZ - 1], 6),
        (rp.at[0 : NY - 1], 7),
        (rd.at[0 : NZ - 1], 8),
        (rx.at[0 : NSHORT - 1], 9),
        (re.at[0 : NSHORT - 1], 10),
        (rf.at[0 : NZ - 1], 11),
    ):
        all_of(ref, phase).wait_send()

    @pl.when(y == owner)
    def _():
        all_of(rd.at[0:12], 12).wait_send()


def body(
    hidden,
    attn_gain,
    query_weight,
    head_bias,
    key_cache,
    value_cache,
    lengths,
    out_weight,
    moe_gain,
    route_group,
    route_inner,
    route_weight,
    gate_w,
    up_w,
    down_w,
):
    vmem = pl.BlockSpec(memory_space=pltpu.VMEM)
    hbm = pl.BlockSpec(memory_space=pltpu.HBM)

    def buf(*shape):
        return pltpu.VMEM(shape, BF16)

    return pl.pallas_call(
        kernel,
        out_shape=jax.ShapeDtypeStruct((4, 512), BF16),
        in_specs=[hbm] * 15,
        out_specs=vmem,
        scratch_shapes=[
            buf(4, 2048),
            pltpu.VMEM((16, 128), F32),
            buf(16, 512),
            pltpu.SMEM((16,), F32),
            pltpu.SMEM((4,), jnp.int32),
            buf(16, 512),
            pltpu.VMEM((16, 128), F32),
            pltpu.SMEM((4,), jnp.int32),
            pltpu.SMEM((2, 4), jnp.int32),
            buf(2, 4),
            buf(4, 1024, 128),
            buf(4, 1024, 128),
            buf(192, 2048),
            buf(192, 2048),
            buf(192, 2048),
            buf(NXC, 16, 512),
            buf(NXC, 16, 512),
            buf(NZ, 8, 128),
            buf(NZ, 8, 128),
            buf(8, 128),
            buf(NZ, 8, 128),
            buf(NZ, 8, 128),
            buf(NZ, 8, 128),
            buf(NZ, 2, 8, 128),
            buf(NZ, 2, 8, 128),
            buf(16, 128),
            buf(NZ, 16, 128),
            buf(NY, 4, 8, 128),
            buf(NY, 4, 8, 128),
            buf(16, 128),
            buf(NZ, 16, 128),
            buf(NXC, 8, 8, 128),
            buf(NSHORT, 8, 8, 128),
            buf(NXC, NY, 2, NY, 8, 128),
            buf(NSHORT, 2, NY, 8, 128),
            buf(NZ, 2, 8, 128),
            buf(NZ, 2, 8, 128),
            buf(4, 16, 128),
            pltpu.SemaphoreType.DMA((15,)),
            pltpu.SemaphoreType.DMA((13,)),
            pltpu.SemaphoreType.DMA((13,)),
        ],
        compiler_params=pltpu.CompilerParams(
            collective_id=0, has_side_effects=True, vmem_limit_bytes=67043328
        ),
        name="layer",
    )(
        hidden,
        attn_gain.reshape(16, 128),
        query_weight,
        head_bias,
        key_cache.reshape(4, 1024, 128),
        value_cache.reshape(4, 1024, 128),
        lengths,
        out_weight.T,
        moe_gain.reshape(16, 128),
        route_group,
        route_inner.T,
        route_weight.T,
        jnp.swapaxes(gate_w, 1, 2).reshape(192, 2048),
        jnp.swapaxes(up_w, 1, 2).reshape(192, 2048),
        down_w.reshape(192, 2048),
    )


def solution(mesh):
    torus = Mesh(mesh.devices.reshape(NZ, NX, NC, NY), ("ep_0", "ep_1", "ep_2", "tp"))
    placed = (
        P(EP, None),
        P(),
        P(EP, "tp"),
        P(),
        P(EP, "tp", None, None),
        P(EP, "tp", None, None),
        P(EP),
        P("tp", EP),
        P(),
        P(EP),
        P(EP, None),
        P(EP, None),
        P(EP, None, "tp"),
        P(EP, None, "tp"),
        P(EP, "tp", None),
    )
    return jax.shard_map(body, mesh=torus, in_specs=placed, out_specs=P(EP, "tp"), check_vma=False)
```

```python
import jax
import jax.numpy as jnp
from jax import lax
from jax.experimental import pallas as pl
from jax.experimental.pallas import tpu as pltpu
from jax.sharding import Mesh
from jax.sharding import PartitionSpec as P

EP = ("ep_0", "ep_1", "ep_2")
MESH = pl.DeviceIdType.MESH
F32 = jnp.float32
BF16 = jnp.bfloat16
NZ, NX, NC, NY = 16, 4, 2, 4
NXC = NX * NC
NSHORT = NXC * NY
EPS = 1e-06

Z_ORDER = (8, 7, 9, 6, 10, 5, 11, 4, 12, 3, 13, 2, 14, 1, 15)
HOPS = (0, 1, 2, 1)
XC_ORDER = sorted(((dx, dc) for dx in range(NX) for dc in range(NC) if dx or dc), key=lambda d: (-HOPS[d[0]], d))
SHORT_ORDER = sorted(
    ((dx, dc, dy) for dx in range(NX) for dc in range(NC) for dy in range(NY) if dx or dc or dy),
    key=lambda d: (-HOPS[d[0]] - HOPS[d[2]], d),
)

NT = (((1,), (1,)), ((), ()))
TN = (((0,), (0,)), ((), ()))


def dot(a, b, dims=None, precision=None):
    if dims is None:
        dims = (((1,), (0,)), ((), ()))
    return lax.dot_general(a, b, dims, precision=precision, preferred_element_type=F32)


def iota(shape, dim):
    return lax.broadcasted_iota(jnp.int32, shape, dim)


def kernel(
    hid_hbm,
    again_hbm,
    wq_hbm,
    bias_hbm,
    k_hbm,
    v_hbm,
    len_hbm,
    wo_hbm,
    mgain_hbm,
    rg_hbm,
    ri_hbm,
    rw_hbm,
    gate_hbm,
    up_hbm,
    down_hbm,
    out_ref,
    hid_ref,
    again_ref,
    wq_ref,
    bias_ref,
    len_ref,
    wo_t,
    mgain_ref,
    rg_ref,
    ri_ref,
    rw_ref,
    k_v,
    v_v,
    wg_v,
    wu_v,
    wd_v,
    wq_g,
    wo_r,
    wo_g,
    sn,
    sh,
    sr,
    rn,
    rh,
    rr,
    sq,
    rq,
    so,
    ro,
    sd,
    rd,
    sx,
    rx,
    se,
    re,
    sf,
    rf,
    load_sem,
    send_sem,
    recv_sem,
):
    z = lax.axis_index("ep_0")
    x = lax.axis_index("ep_1")
    c = lax.axis_index("ep_2")
    y = lax.axis_index("tp")
    xc = x * NC + c
    me = xc * NY + y

    def z_at(off):
        return lax.rem(z + off, NZ)

    def xc_at(dx, dc):
        return lax.rem(x + dx, NX), lax.rem(c + dc, NC)

    def y_at(dy):
        return lax.rem(y + dy, NY)

    barrier = pltpu.get_barrier_semaphore()

    def greet(device):
        pl.semaphore_signal(barrier, inc=1, device_id=device, device_id_type=MESH)

    for off in Z_ORDER:
        greet((z_at(off), x, c, y))
    for dx, dc in XC_ORDER:
        greet((z, *xc_at(dx, dc), y))
    for dy in range(1, NY):
        greet((z, x, c, y_at(dy)))
    greeted = NZ - 1 + NXC - 1 + NY - 1

    copies = (
        (hid_hbm, hid_ref),
        (again_hbm, again_ref),
        (rw_hbm, rw_ref),
        (rg_hbm, rg_ref),
        (ri_hbm, ri_ref),
        (wq_hbm, wq_ref),
        (wo_hbm, wo_t),
        (bias_hbm, bias_ref),
        (len_hbm, len_ref),
        (mgain_hbm, mgain_ref),
        (k_hbm, k_v),
        (v_hbm, v_v),
        (gate_hbm, wg_v),
        (up_hbm, wu_v),
        (down_hbm, wd_v),
    )
    loads = [pltpu.make_async_copy(src, dst, load_sem.at[i]) for i, (src, dst) in enumerate(copies)]
    for one in loads:
        one.start()
    for one in loads[0:5]:
        one.wait()

    hid = hid_ref[...].astype(F32)
    scale = lax.rsqrt(jnp.mean(hid * hid, axis=-1, keepdims=True) + EPS)
    hid2 = jnp.concatenate([hid, hid], axis=0)
    scale2 = jnp.concatenate([scale, scale], axis=0)
    for k in range(NZ):
        part = hid2[:, 128 * k : 128 * k + 128]
        sn[k] = (part * scale2 * again_ref[k : k + 1, :]).astype(BF16)
        sh[k] = part.astype(BF16)

    lane = iota((1, 128), 1)
    tok_a = lane % 4
    near = (lane % 64) // 4 == z
    wide = lane // 8 == z
    route_w = rw_ref[...].astype(F32)
    rows = []
    for pattern in (near, wide):
        for k in range(2):
            row = jnp.zeros((1, 128), F32)
            for t in range(4):
                ident = (rg_ref[t] * 32 + ri_ref[k, t]).astype(F32)
                row = jnp.where(tok_a == t, ident, row)
            rows.append(jnp.where(pattern, row, 0.0))
    for k in range(2):
        row = jnp.zeros((1, 128), F32)
        for t in range(4):
            row = jnp.where(tok_a == t, route_w[k : k + 1, t : t + 1], row)
        rows.append(jnp.where(wide, row, 0.0))
    rowid = iota((8, 128), 0)
    packet = jnp.zeros((8, 128), F32)
    for k, row in enumerate(rows):
        packet = jnp.where(rowid == k, jnp.broadcast_to(row, (8, 128)), packet)
    sr[...] = packet.astype(BF16)

    for one in loads[5:10]:
        one.wait()
    pl.semaphore_wait(barrier, greeted)

    def send(device, src, dst, phase):
        pltpu.make_async_remote_copy(
            src_ref=src,
            dst_ref=dst,
            send_sem=send_sem.at[phase],
            recv_sem=recv_sem.at[phase],
            device_id=device,
            device_id_type=MESH,
        ).start()

    def all_of(ref, phase):
        return pltpu.make_async_remote_copy(
            src_ref=ref,
            dst_ref=ref,
            send_sem=send_sem.at[phase],
            recv_sem=recv_sem.at[phase],
            device_id=(z_at(1), x, c, y),
            device_id_type=MESH,
        )

    def gather_line(src_of, dst, phase):
        for off in Z_ORDER:
            send((z_at(off), x, c, y), src_of(off), dst.at[NZ - off], phase)

    gather_line(lambda off: sn.at[z_at(off)], rn, 0)
    for dx, dc in XC_ORDER:
        send((z, *xc_at(dx, dc), y), wq_ref, wq_g.at[xc], 1)
    quad = lax.div(z, 4)
    for off in (8, 4, 12):
        send((z_at(off), x, c, y), wo_t, wo_r.at[quad], 4)
    gather_line(lambda off: sr, rr, 3)

    def near_chunk(off):
        return lax.rem(z + off, 4) + 4 * y

    for i in range(4):
        if i != 2:
            off = (2 - i) % NZ
            send((z_at(off), x, c, y), sh.at[near_chunk(off)], rh.at[i], 2)
    rn[0] = sn[z]
    rr[0] = sr[...]
    rh[2] = sh[near_chunk(0)]
    wq_g[xc] = wq_ref[...]
    wo_r[quad] = wo_t[...]

    all_of(rn.at[1:NZ], 0).wait_recv()
    all_of(wq_g.at[1:NXC], 1).wait_recv()

    first = (iota((128, 128), 0) % 8) < 4
    xin = rn[...].astype(F32).reshape(128, 128).astype(BF16)
    part_q = dot(xin, wq_g[...].reshape(128, 512))
    for p in range(2):
        pair = jnp.where(first, part_q[:, 256 * p : 256 * p + 128], part_q[:, 256 * p + 128 : 256 * p + 256])
        sq[:, p] = pair.reshape(NZ, 8, 128).astype(BF16)
    gather_line(lambda off: sq.at[off], rq, 5)
    rq[0] = sq[0]

    all_of(wo_r.at[1:4], 4).wait_recv()
    for dx, dc, dy in SHORT_ORDER:
        p = y_at(dy)
        send((z, *xc_at(dx, dc), p), wo_r.at[p], wo_g.at[y * NXC + xc], 7)
    wo_g[y * NXC + xc] = wo_r[y]

    later = (iota((128, 128), 0) > iota((128, 128), 1)).astype(F32)
    rowh = iota((16, 1), 0)
    bias = jnp.zeros((16, 1), F32)
    length = jnp.zeros((16, 1), jnp.int32)
    for h in range(4):
        bias = jnp.where(rowh // 4 == h, bias_ref[4 * y + h], bias)
        length = jnp.where(rowh % 4 == h, len_ref[h], length)

    all_of(rq.at[1:NZ], 5).wait_recv()
    q = jnp.sum(rq[...].astype(F32), axis=0).reshape(16, 128).astype(BF16)
    loads[10].wait()
    tok = iota((16, 1024), 0) % 4
    scores = jnp.zeros((16, 1024), F32)
    for t in range(4):
        scores = jnp.where(tok == t, dot(q, k_v[t], NT), scores)
    scores = scores * (128.0 ** -0.5) + bias
    soft = jnp.log1p(jnp.exp(-jnp.abs(scores)))
    log_stop = jnp.minimum(scores, 0.0) - soft
    visible = iota((16, 1024), 1) < length
    log_keep = jnp.where(visible, log_stop - scores, 0.0)
    stacked = jnp.concatenate([log_keep[:, 128 * k : 128 * k + 128] for k in range(8)], axis=0)
    within = dot(stacked, later, precision=lax.Precision.HIGHEST)
    carry_sum = jnp.zeros((16, 1), F32)
    weights = [None] * 8
    for k in reversed(range(8)):
        inner = within[16 * k : 16 * k + 16]
        keep_k = log_keep[:, 128 * k : 128 * k + 128]
        expo = jnp.exp(log_stop[:, 128 * k : 128 * k + 128] + (inner + carry_sum))
        weights[k] = jnp.where(visible[:, 128 * k : 128 * k + 128], expo, 0.0)
        carry_sum = carry_sum + (inner[:, 0:1] + keep_k[:, 0:1])
    weight = jnp.concatenate(weights, axis=1).astype(BF16)
    loads[11].wait()
    tok_o = iota((16, 128), 0) % 4
    heads = jnp.zeros((16, 128), F32)
    for t in range(4):
        heads = jnp.where(tok_o == t, dot(weight, v_v[t]), heads)
    so[...] = heads.astype(BF16)

    for dy in (2, 1, 3, 0):
        for i in (0, 1, 3, 2):
            if dy or i != 2:
                send((z_at((2 - i) % NZ), x, c, y_at(dy)), so, ro.at[4 * y + i], 6)
    ro[4 * y + 2] = so[...]

    all_of(rr.at[1:NZ], 3).wait_recv()
    route = jnp.sum(rr[...].astype(F32), axis=0)
    ids = pltpu.roll(route, lax.rem(4 * (NZ + 4 - z), 128), 1)
    wides = pltpu.roll(route, lax.rem(8 * (NZ + 4 - z), 128), 1)

    def select_of(g, start, count):
        shape = (64, 16 * count)
        row = iota(shape, 0)
        expert = (NXC * z + row // 8).astype(F32)
        same = iota(shape, 1) // 4 + (start - 6) == 8 * g + row % 8
        own = pltpu.roll(ids, (4 * (6 - start)) % 128, 1)
        wanted = (own[0:1, 0 : 16 * count] == expert) | (own[1:2, 0 : 16 * count] == expert)
        return jnp.where(same & wanted, 1.0, 0.0).astype(BF16)

    starts = ((4, 3), (5, 3), (6, 2), (3, 3))
    selects = [[select_of(g, start + 8 * g, count) for start, count in starts] for g in range(2)]

    def combine_of(g):
        row = iota((128, 64), 0)
        col = iota((128, 64), 1)
        expert = (NXC * z + (row // 8) % NXC).astype(F32)
        same = (row % 8 == col // 8) & (row // 64 == (col // 4) % 2)
        own = wides[:, 64 * g : 64 * g + 64]
        weight = jnp.where(own[2:3] == expert, own[4:5], 0.0) + jnp.where(own[3:4] == expert, own[5:6], 0.0)
        return jnp.where(same, weight, 0.0).astype(BF16)

    combines = [combine_of(g) for g in range(2)]

    all_of(rh.at[1:4], 2).wait_recv()
    all_of(wo_g.at[1:NSHORT], 7).wait_recv()
    all_of(ro.at[1:NZ], 6).wait_recv()
    head_row = (iota((64, 128), 0) % 16) // 4
    resid = rh[...].astype(F32)
    for p in range(NY):
        heads_in = ro[4 * p : 4 * p + 4].reshape(64, 128)
        wo_p = wo_g[NXC * p : NXC * p + NXC].reshape(128, 512)
        proj = jnp.zeros((64, 128), F32)
        for h in range(4):
            proj = jnp.where(head_row == h, dot(heads_in, wo_p[:, 128 * h : 128 * h + 128], NT), proj)
        proj = jnp.sum(proj.reshape(4, 2, 8, 128), axis=1)
        proj = proj + pltpu.roll(proj, 4, 1)
        resid = resid + proj.astype(BF16).astype(F32)
    first8 = iota((8, 128), 0) < 4
    sd[...] = jnp.concatenate(
        [jnp.where(first8, resid[0], resid[1]), jnp.where(first8, resid[2], resid[3])], axis=0
    ).astype(BF16)

    for off in Z_ORDER:
        send((z_at(off), x, c, y), sd, rd.at[(8 - off) % NZ], 12 if 6 <= off <= 10 else 8)
    rd[8] = sd[...]

    def to_experts(g, phase):
        for q, (start, count) in enumerate(starts):
            rows = jnp.concatenate([rd[(start + 8 * g + 4 * k) % NZ] for k in range(count)], axis=0)
            slots = dot(selects[g][q], rows).reshape(NXC, 1, 8, 128).astype(BF16)
            sx[:, g, pl.ds(lax.rem(z + q, 4), 1)] = slots
        for dx, dc, dy in SHORT_ORDER:
            px, pc = xc_at(dx, dc)
            send((z, px, pc, y_at(dy)), sx.at[px * NC + pc, g], rx.at[g, me], phase)
        rx[g, me] = sx[xc, g]

    all_of(rd.at[1:11], 8).wait_recv()
    to_experts(0, 9)
    all_of(rd.at[1:6], 12).wait_recv()
    to_experts(1, 13)

    pieces = [rd[10 - i].astype(F32)[4 * i : 4 * i + 4] for i in range(4)]
    own_rows = []
    for k in range(4):
        row = jnp.zeros((4, 128), F32)
        for i in range(4):
            row = jnp.where(lax.rem(z + 10 - i, 4) == k, pieces[i], row)
        own_rows.append(row)

    for one in loads[12:]:
        one.wait()
    all_of(rx.at[0, 1:NSHORT], 9).wait_recv()
    all_of(rx.at[1, 1:NSHORT], 13).wait_recv()
    rx_v = rx.reshape(2, NXC, NY, 4, 8, 128)
    chunks = [rx_v[:, :, k // 4, k % 4].astype(F32).reshape(128, 128) for k in range(16)]
    square = chunks[0] * chunks[0]
    for k in range(1, 16):
        square = square + chunks[k] * chunks[k]
    scale_two = lax.rsqrt(jnp.sum(square, axis=-1, keepdims=True) * (1.0 / 2048.0) + EPS)
    lhs = jnp.concatenate(
        [(chunks[k] * scale_two * mgain_ref[k : k + 1, :]).astype(BF16) for k in range(16)], axis=1
    )
    gated = dot(lhs, wg_v[...], NT)
    upped = dot(lhs, wu_v[...], NT)
    act = (gated / (1.0 + jnp.exp(-gated)) * upped).astype(BF16)
    for p in range(NY):
        down = dot(act, wd_v[:, 512 * p : 512 * p + 512])
        for k in range(4):
            se[:, :, p, k] = down[:, 128 * k : 128 * k + 128].reshape(2, NXC, 8, 128).astype(BF16)

    for g, phase in ((1, 10), (0, 14)):
        for dx, dc, dy in SHORT_ORDER:
            px, pc = xc_at(dx, dc)
            p = y_at(dy)
            send((z, px, pc, p), se.at[g, px * NC + pc, p], re.at[g, me], phase)
        re[g, me] = se[g, xc, y]

    re_v = re.reshape(2, NXC, NY, 4, 8, 128)

    def to_tokens(g):
        totals = []
        for k in range(4):
            total = re_v[g, :, 0, k].astype(F32)
            for p in range(1, NY):
                total = total + re_v[g, :, p, k].astype(F32)
            totals.append(total.reshape(64, 128).astype(BF16))
        for p in range(2):
            mixed = dot(combines[g], jnp.concatenate(totals[2 * p : 2 * p + 2], axis=0), TN)
            sf[g, :, p] = mixed.reshape(8, 8, 128).astype(BF16)
        for b in (4, 3, 5, 2, 6, 1, 7, 0) if g else (0, 7, 1, 6, 2, 5, 3, 4):
            off = (b - 4 + 8 * g) % NZ
            if off:
                send((z_at(off), x, c, y), sf.at[g, b], rf.at[NZ - off], 11)

    all_of(re.at[1, 1:NSHORT], 10).wait_recv()
    to_tokens(1)
    all_of(re.at[0, 1:NSHORT], 14).wait_recv()
    to_tokens(0)
    rf[0] = sf[0, 4]

    all_of(rf.at[1:NZ], 11).wait_recv()
    routed = jnp.sum(rf[...].astype(F32), axis=0).reshape(16, 128)
    for k in range(4):
        out_ref[:, 128 * k : 128 * k + 128] = (own_rows[k] + routed[4 * k : 4 * k + 4]).astype(BF16)

    for ref, phase in (
        (rn.at[1:NZ], 0),
        (wq_g.at[1:NXC], 1),
        (rh.at[1:4], 2),
        (rr.at[1:NZ], 3),
        (wo_r.at[1:4], 4),
        (rq.at[1:NZ], 5),
        (ro.at[1:NZ], 6),
        (wo_g.at[1:NSHORT], 7),
        (rd.at[1:11], 8),
        (rx.at[0, 1:NSHORT], 9),
        (re.at[1, 1:NSHORT], 10),
        (rf.at[1:NZ], 11),
        (rd.at[1:6], 12),
        (rx.at[1, 1:NSHORT], 13),
        (re.at[0, 1:NSHORT], 14),
    ):
        all_of(ref, phase).wait_send()


def body(
    hidden,
    attn_gain,
    query_weight,
    head_bias,
    key_cache,
    value_cache,
    lengths,
    out_weight,
    moe_gain,
    route_group,
    route_inner,
    route_weight,
    gate_w,
    up_w,
    down_w,
):
    vmem = pl.BlockSpec(memory_space=pltpu.VMEM)
    hbm = pl.BlockSpec(memory_space=pltpu.HBM)

    def buf(*shape):
        return pltpu.VMEM(shape, BF16)

    return pl.pallas_call(
        kernel,
        out_shape=jax.ShapeDtypeStruct((4, 512), BF16),
        in_specs=[hbm] * 15,
        out_specs=vmem,
        scratch_shapes=[
            buf(4, 2048),
            pltpu.VMEM((16, 128), F32),
            buf(16, 512),
            pltpu.SMEM((16,), F32),
            pltpu.SMEM((4,), jnp.int32),
            buf(16, 512),
            pltpu.VMEM((16, 128), F32),
            pltpu.SMEM((4,), jnp.int32),
            pltpu.SMEM((2, 4), jnp.int32),
            buf(2, 4),
            buf(4, 1024, 128),
            buf(4, 1024, 128),
            buf(192, 2048),
            buf(192, 2048),
            buf(192, 2048),
            buf(NXC, 16, 512),
            buf(4, 16, 512),
            buf(NSHORT, 16, 512),
            buf(NZ, 8, 128),
            buf(NZ, 8, 128),
            buf(8, 128),
            buf(NZ, 8, 128),
            buf(4, 8, 128),
            buf(NZ, 8, 128),
            buf(NZ, 2, 8, 128),
            buf(NZ, 2, 8, 128),
            buf(16, 128),
            buf(NZ, 16, 128),
            buf(16, 128),
            buf(NZ, 16, 128),
            buf(NXC, 2, 4, 8, 128),
            buf(2, NSHORT, 4, 8, 128),
            buf(2, NXC, NY, 4, 8, 128),
            buf(2, NSHORT, 4, 8, 128),
            buf(2, 8, 2, 8, 128),
            buf(NZ, 2, 8, 128),
            pltpu.SemaphoreType.DMA((15,)),
            pltpu.SemaphoreType.DMA((15,)),
            pltpu.SemaphoreType.DMA((15,)),
        ],
        compiler_params=pltpu.CompilerParams(
            collective_id=0, has_side_effects=True, vmem_limit_bytes=67043328
        ),
        name="layer",
    )(
        hidden,
        attn_gain.reshape(16, 128),
        query_weight,
        head_bias,
        key_cache.reshape(4, 1024, 128),
        value_cache.reshape(4, 1024, 128),
        lengths,
        out_weight.T,
        moe_gain.reshape(16, 128),
        route_group,
        route_inner.T,
        route_weight.T,
        jnp.swapaxes(gate_w, 1, 2).reshape(192, 2048),
        jnp.swapaxes(up_w, 1, 2).reshape(192, 2048),
        down_w.reshape(192, 2048),
    )


def solution(mesh):
    torus = Mesh(mesh.devices.reshape(NZ, NX, NC, NY), ("ep_0", "ep_1", "ep_2", "tp"))
    placed = (
        P(EP, None),
        P(),
        P(EP, "tp"),
        P(),
        P(EP, "tp", None, None),
        P(EP, "tp", None, None),
        P(EP),
        P("tp", EP),
        P(),
        P(EP),
        P(EP, None),
        P(EP, None),
        P(EP, None, "tp"),
        P(EP, None, "tp"),
        P(EP, "tp", None),
    )
    return jax.shard_map(body, mesh=torus, in_specs=placed, out_specs=P(EP, "tp"), check_vma=False)
```

```python
import jax
import jax.numpy as jnp
from jax import lax
from jax.experimental import pallas as pl
from jax.experimental.pallas import tpu as pltpu
from jax.sharding import Mesh
from jax.sharding import PartitionSpec as P

EP = ("ep_0", "ep_1", "ep_2")
MESH = pl.DeviceIdType.MESH
F32 = jnp.float32
BF16 = jnp.bfloat16
NZ, NX, NC, NY = 16, 4, 2, 4
NXC = NX * NC
NSHORT = NXC * NY
EPS = 1e-06

Z_ORDER = (8, 7, 9, 6, 10, 5, 11, 4, 12, 3, 13, 2, 14, 1, 15)
NEAR_ORDER = (4, 12, 3, 13, 2, 14, 1, 15)
HOPS = (0, 1, 2, 1)
XC_ORDER = sorted(((dx, dc) for dx in range(NX) for dc in range(NC) if dx or dc), key=lambda d: (-HOPS[d[0]], d))
SHORT_ORDER = sorted(
    ((dx, dc, dy) for dx in range(NX) for dc in range(NC) for dy in range(NY) if dx or dc or dy),
    key=lambda d: (-HOPS[d[0]] - HOPS[d[2]], d),
)

NT = (((1,), (1,)), ((), ()))
TN = (((0,), (0,)), ((), ()))


def dot(a, b, dims=None, precision=None):
    if dims is None:
        dims = (((1,), (0,)), ((), ()))
    return lax.dot_general(a, b, dims, precision=precision, preferred_element_type=F32)


def iota(shape, dim):
    return lax.broadcasted_iota(jnp.int32, shape, dim)


def kernel(
    hid_hbm,
    again_hbm,
    wq_hbm,
    bias_hbm,
    k_hbm,
    v_hbm,
    len_hbm,
    wo_hbm,
    mgain_hbm,
    rg_hbm,
    ri_hbm,
    rw_hbm,
    gate_hbm,
    up_hbm,
    down_hbm,
    out_ref,
    hid_ref,
    again_ref,
    wq_ref,
    bias_ref,
    len_ref,
    wo_t,
    mgain_ref,
    rg_ref,
    ri_ref,
    rw_ref,
    k_v,
    v_v,
    wg_v,
    wu_v,
    wd_v,
    wq_r,
    wq_g,
    wo_r,
    wo_g,
    sn,
    st,
    sh,
    sr,
    rn,
    rh,
    rr,
    sq,
    rq,
    so,
    ro,
    sd,
    rd,
    sx,
    rx,
    se,
    re,
    sf,
    rf,
    load_sem,
    send_sem,
    recv_sem,
):
    z = lax.axis_index("ep_0")
    x = lax.axis_index("ep_1")
    c = lax.axis_index("ep_2")
    y = lax.axis_index("tp")
    xc = x * NC + c
    me = xc * NY + y

    def z_at(off):
        return lax.rem(z + off, NZ)

    def xc_at(dx, dc):
        return lax.rem(x + dx, NX), lax.rem(c + dc, NC)

    def y_at(dy):
        return lax.rem(y + dy, NY)

    barrier = pltpu.get_barrier_semaphore()

    def greet(device):
        pl.semaphore_signal(barrier, inc=1, device_id=device, device_id_type=MESH)

    for off in NEAR_ORDER:
        greet((z_at(off), x, c, y))
    for dx, dc in XC_ORDER:
        greet((z, *xc_at(dx, dc), y))
    for dy in range(1, NY):
        greet((z, x, c, y_at(dy)))
    greeted = len(NEAR_ORDER) + NXC - 1 + NY - 1

    copies = (
        (hid_hbm, hid_ref),
        (again_hbm, again_ref),
        (rw_hbm, rw_ref),
        (rg_hbm, rg_ref),
        (ri_hbm, ri_ref),
        (wq_hbm, wq_ref),
        (wo_hbm, wo_t),
        (bias_hbm, bias_ref),
        (len_hbm, len_ref),
        (mgain_hbm, mgain_ref),
        (k_hbm, k_v),
        (v_hbm, v_v),
        (gate_hbm, wg_v),
        (up_hbm, wu_v),
        (down_hbm, wd_v),
    )
    loads = [pltpu.make_async_copy(src, dst, load_sem.at[i]) for i, (src, dst) in enumerate(copies)]
    for one in loads:
        one.start()
    for one in loads[0:5]:
        one.wait()

    hid = hid_ref[...].astype(F32)
    scale = lax.rsqrt(jnp.mean(hid * hid, axis=-1, keepdims=True) + EPS)
    hid2 = jnp.concatenate([hid, hid], axis=0)
    scale2 = jnp.concatenate([scale, scale], axis=0)
    for k in range(NZ):
        part = hid2[:, 128 * k : 128 * k + 128]
        sn[k] = (part * scale2 * again_ref[k : k + 1, :]).astype(BF16)
        sh[k] = part.astype(BF16)
    first8 = iota((8, 128), 0) < 4
    for i in range(8):
        st[i] = jnp.where(first8, sn[z_at(i)].astype(F32), sn[z_at(i + 8)].astype(F32)).astype(BF16)

    lane = iota((1, 128), 1)
    tok_a = lane % 4
    near = (lane % 64) // 4 == z
    wide = lane // 8 == z
    route_w = rw_ref[...].astype(F32)
    rows = []
    for pattern in (near, wide):
        for k in range(2):
            row = jnp.zeros((1, 128), F32)
            for t in range(4):
                ident = (rg_ref[t] * 32 + ri_ref[k, t]).astype(F32)
                row = jnp.where(tok_a == t, ident, row)
            rows.append(jnp.where(pattern, row, 0.0))
    for k in range(2):
        row = jnp.zeros((1, 128), F32)
        for t in range(4):
            row = jnp.where(tok_a == t, route_w[k : k + 1, t : t + 1], row)
        rows.append(jnp.where(wide, row, 0.0))
    rowid = iota((8, 128), 0)
    packet = jnp.zeros((8, 128), F32)
    for k, row in enumerate(rows):
        packet = jnp.where(rowid == k, jnp.broadcast_to(row, (8, 128)), packet)
    sr[...] = packet.astype(BF16)

    for one in loads[5:10]:
        one.wait()
    pl.semaphore_wait(barrier, greeted)

    def send(device, src, dst, phase):
        pltpu.make_async_remote_copy(
            src_ref=src,
            dst_ref=dst,
            send_sem=send_sem.at[phase],
            recv_sem=recv_sem.at[phase],
            device_id=device,
            device_id_type=MESH,
        ).start()

    def all_of(ref, phase):
        return pltpu.make_async_remote_copy(
            src_ref=ref,
            dst_ref=ref,
            send_sem=send_sem.at[phase],
            recv_sem=recv_sem.at[phase],
            device_id=(z_at(1), x, c, y),
            device_id_type=MESH,
        )

    send((z_at(12), x, c, y), wq_ref, wq_r.at[0], 1)
    send((z_at(4), x, c, y), wq_ref, wq_r.at[1], 12)
    for i in (0, 1, 7, 2, 6, 3, 5):
        send((z_at((i - 4) % NZ), x, c, y), st.at[i], rn.at[i], 0)
    for slot, off in ((1, 12), (3, 4)):
        send((z_at(off), x, c, y), wo_t, wo_r.at[slot], 4)

    def near_chunk(off):
        return lax.rem(z + off, 4) + 4 * y

    for i in range(4):
        if i != 2:
            off = (2 - i) % NZ
            send((z_at(off), x, c, y), sh.at[near_chunk(off)], rh.at[i], 2)
    rn[4] = st[4]
    rr[0] = sr[...]
    rh[2] = sh[near_chunk(0)]
    wo_r[0] = wo_t[...]

    quad = lax.div(z, 4)

    def gather_rows(slot, phase):
        all_of(wq_r.at[0], phase).wait_recv()
        for dx, dc in XC_ORDER:
            send((z, *xc_at(dx, dc), y), wq_r.at[slot], wq_g.at[xc, slot], 15)

    @pl.when(lax.rem(quad, 2) == 0)
    def _():
        gather_rows(0, 1)
        gather_rows(1, 12)

    @pl.when(lax.rem(quad, 2) == 1)
    def _():
        gather_rows(1, 12)
        gather_rows(0, 1)

    wq_g[xc] = wq_r[...]
    all_of(wo_r.at[0:2], 4).wait_recv()
    send((z_at(12), x, c, y), wo_r.at[1], wo_r.at[2], 16)
    for off in Z_ORDER:
        send((z_at(off), x, c, y), sr, rr.at[NZ - off], 3)
    all_of(rn.at[1:8], 0).wait_recv()
    xin = rn[...].astype(F32).reshape(64, 128).astype(BF16)
    all_of(wq_g.at[1:NXC], 15).wait_recv()

    first_q = (iota((64, 512), 0) % 8) < 4
    part_q = jnp.where(
        first_q, dot(xin, wq_g[:, 0].reshape(128, 512)), dot(xin, wq_g[:, 1].reshape(128, 512))
    ).reshape(8, 8, 512)
    part_q = (part_q + pltpu.roll(part_q, 4, 1)).reshape(64, 512)
    first = first_q[:, 0:128]
    for p in range(2):
        pair = jnp.where(first, part_q[:, 256 * p : 256 * p + 128], part_q[:, 256 * p + 128 : 256 * p + 256])
        sq[:, p] = pair.reshape(8, 8, 128).astype(BF16)
    for i in (0, 1, 7, 2, 6, 3, 5):
        send((z_at((4 - i) % NZ), x, c, y), sq.at[i], rq.at[i], 5)
    rq[4] = sq[4]


    def share(slot):
        p = lax.rem(quad + slot, NY)
        for dx, dc in XC_ORDER:
            send((z, *xc_at(dx, dc), p), wo_r.at[slot], wo_g.at[y * NXC + xc], 7)

        @pl.when(p != y)
        def _():
            send((z, x, c, p), wo_r.at[slot], wo_g.at[y * NXC + xc], 7)

        @pl.when(p == y)
        def _():
            wo_g[y * NXC + xc] = wo_r[slot]

    for slot in (0, 1, 3):
        share(slot)

    later = (iota((128, 128), 0) > iota((128, 128), 1)).astype(F32)
    rowh = iota((16, 1), 0)
    bias = jnp.zeros((16, 1), F32)
    length = jnp.zeros((16, 1), jnp.int32)
    for h in range(4):
        bias = jnp.where(rowh // 4 == h, bias_ref[4 * y + h], bias)
        length = jnp.where(rowh % 4 == h, len_ref[h], length)

    all_of(wo_r.at[0:1], 16).wait_recv()
    share(2)
    all_of(rq.at[1:8], 5).wait_recv()
    q = jnp.sum(rq[...].astype(F32), axis=0).reshape(16, 128).astype(BF16)
    loads[10].wait()
    tok = iota((16, 1024), 0) % 4
    scores = jnp.zeros((16, 1024), F32)
    for t in range(4):
        scores = jnp.where(tok == t, dot(q, k_v[t], NT), scores)
    scores = scores * (128.0 ** -0.5) + bias
    soft = jnp.log1p(jnp.exp(-jnp.abs(scores)))
    log_stop = jnp.minimum(scores, 0.0) - soft
    visible = iota((16, 1024), 1) < length
    log_keep = jnp.where(visible, log_stop - scores, 0.0)
    stacked = jnp.concatenate([log_keep[:, 128 * k : 128 * k + 128] for k in range(8)], axis=0)
    within = dot(stacked, later, precision=lax.Precision.HIGHEST)
    carry_sum = jnp.zeros((16, 1), F32)
    weights = [None] * 8
    for k in reversed(range(8)):
        inner = within[16 * k : 16 * k + 16]
        keep_k = log_keep[:, 128 * k : 128 * k + 128]
        expo = jnp.exp(log_stop[:, 128 * k : 128 * k + 128] + (inner + carry_sum))
        weights[k] = jnp.where(visible[:, 128 * k : 128 * k + 128], expo, 0.0)
        carry_sum = carry_sum + (inner[:, 0:1] + keep_k[:, 0:1])
    weight = jnp.concatenate(weights, axis=1).astype(BF16)
    loads[11].wait()
    tok_o = iota((16, 128), 0) % 4
    heads = jnp.zeros((16, 128), F32)
    for t in range(4):
        heads = jnp.where(tok_o == t, dot(weight, v_v[t]), heads)
    so[...] = heads.astype(BF16)

    for dy in (2, 1, 3, 0):
        for i in (0, 1, 3, 2):
            if dy or i != 2:
                send((z_at((2 - i) % NZ), x, c, y_at(dy)), so, ro.at[4 * y + i], 6)
    ro[4 * y + 2] = so[...]

    all_of(rh.at[1:4], 2).wait_recv()
    all_of(wo_g.at[1:NSHORT], 7).wait_recv()
    all_of(ro.at[1:NZ], 6).wait_recv()
    head_row = (iota((64, 128), 0) % 16) // 4
    resid = rh[...].astype(F32)
    for p in range(NY):
        heads_in = ro[4 * p : 4 * p + 4].reshape(64, 128)
        wo_p = wo_g[NXC * p : NXC * p + NXC].reshape(128, 512)
        proj = jnp.zeros((64, 128), F32)
        for h in range(4):
            proj = jnp.where(head_row == h, dot(heads_in, wo_p[:, 128 * h : 128 * h + 128], NT), proj)
        proj = jnp.sum(proj.reshape(4, 2, 8, 128), axis=1)
        proj = proj + pltpu.roll(proj, 4, 1)
        resid = resid + proj.astype(BF16).astype(F32)
    sd[...] = jnp.concatenate(
        [jnp.where(first8, resid[0], resid[1]), jnp.where(first8, resid[2], resid[3])], axis=0
    ).astype(BF16)

    for off in Z_ORDER:
        send((z_at(off), x, c, y), sd, rd.at[z], 8)
    rd[z] = sd[...]

    all_of(rr.at[1:NZ], 3).wait_recv()
    route = jnp.sum(rr[...].astype(F32), axis=0)

    def select_of(start, count, g):
        shape = (64, 16 * count)
        row = iota(shape, 0)
        expert = (NXC * z + row // 8).astype(F32)
        same = iota(shape, 1) // 4 + (start - 2) == 8 * g + row % 8
        own = pltpu.roll(route, (4 * (2 - start)) % 128, 1)
        wanted = (own[0:1, 0 : 16 * count] == expert) | (own[1:2, 0 : 16 * count] == expert)
        return jnp.where(same & wanted, 1.0, 0.0).astype(BF16)

    starts = ((0, 3), (1, 3), (2, 2), (-1, 3))
    selects = [[select_of(start + 8 * g, count, g) for start, count in starts] for g in range(2)]

    def combine_of(g):
        row = iota((128, 64), 0)
        col = iota((128, 64), 1)
        expert = (NXC * z + (row // 8) % NXC).astype(F32)
        same = (row % 8 == col // 8) & (row // 64 == (col // 4) % 2)
        own = route[:, 64 * g : 64 * g + 64]
        weight = jnp.where(own[2:3] == expert, own[4:5], 0.0) + jnp.where(own[3:4] == expert, own[5:6], 0.0)
        return jnp.where(same, weight, 0.0).astype(BF16)

    combines = [combine_of(g) for g in range(2)]

    def to_experts(g, phase):
        for k, (start, count) in enumerate(starts):
            rows = jnp.concatenate([rd[(start + 8 * g + 4 * n) % NZ] for n in range(count)], axis=0)
            sx[:, g, k] = dot(selects[g][k], rows).reshape(NXC, 8, 128).astype(BF16)
        for dx, dc, dy in SHORT_ORDER:
            px, pc = xc_at(dx, dc)
            send((z, px, pc, y_at(dy)), sx.at[px * NC + pc, g], rx.at[g, me], phase)
        rx[g, me] = sx[xc, g]

    all_of(rd.at[1:NZ], 8).wait_recv()
    to_experts(0, 9)
    to_experts(1, 13)

    pieces = [rd[z_at(18 - i)].astype(F32)[4 * i : 4 * i + 4] for i in range(4)]
    own_rows = []
    for k in range(4):
        row = jnp.zeros((4, 128), F32)
        for i in range(4):
            row = jnp.where(lax.rem(z + 18 - i, 4) == k, pieces[i], row)
        own_rows.append(row)

    rx_v = rx.reshape(2, NXC, NY, 4, 8, 128)
    re_v = re.reshape(2, NXC, NY, 4, 8, 128)

    def experts(g, phase):
        chunks = [rx_v[g, :, k // 4, k % 4].astype(F32).reshape(64, 128) for k in range(16)]
        square = chunks[0] * chunks[0]
        for k in range(1, 16):
            square = square + chunks[k] * chunks[k]
        scale_two = lax.rsqrt(jnp.sum(square, axis=-1, keepdims=True) * (1.0 / 2048.0) + EPS)
        lhs = jnp.concatenate(
            [(chunks[k] * scale_two * mgain_ref[k : k + 1, :]).astype(BF16) for k in range(16)], axis=1
        )
        gated = dot(lhs, wg_v[...], NT)
        upped = dot(lhs, wu_v[...], NT)
        act = (gated / (1.0 + jnp.exp(-gated)) * upped).astype(BF16)
        for p in range(NY):
            down = dot(act, wd_v[:, 512 * p : 512 * p + 512])
            for k in range(4):
                se[g, :, p, k] = down[:, 128 * k : 128 * k + 128].reshape(NXC, 8, 128).astype(BF16)
        for dx, dc, dy in SHORT_ORDER:
            px, pc = xc_at(dx, dc)
            p = y_at(dy)
            send((z, px, pc, p), se.at[g, px * NC + pc, p], re.at[g, me], phase)
        re[g, me] = se[g, xc, y]

    half = lax.div(z, 8)

    def to_tokens(g):
        totals = []
        for k in range(4):
            total = re_v[g, :, 0, k].astype(F32)
            for p in range(1, NY):
                total = total + re_v[g, :, p, k].astype(F32)
            totals.append(total.reshape(64, 128).astype(BF16))
        for p in range(2):
            mixed = dot(combines[g], jnp.concatenate(totals[2 * p : 2 * p + 2], axis=0), TN)
            sf[g, :, p] = mixed.reshape(8, 8, 128).astype(BF16)

        def back(j):
            b = lax.rem(z + j, 8)
            send((8 * g + b, x, c, y), sf.at[g, b], rf.at[z], 11)

        @pl.when(half != g)
        def _():
            back(0)

        for j in (4, 3, 5, 2, 6, 1, 7):
            back(j)

    for one in loads[12:]:
        one.wait()
    all_of(rx.at[0, 1:NSHORT], 9).wait_recv()
    experts(0, 10)
    all_of(rx.at[1, 1:NSHORT], 13).wait_recv()
    experts(1, 14)
    all_of(re.at[0, 1:NSHORT], 10).wait_recv()
    to_tokens(0)
    all_of(re.at[1, 1:NSHORT], 14).wait_recv()
    to_tokens(1)
    rf[z] = sf[half, lax.rem(z, 8)]

    all_of(rf.at[1:NZ], 11).wait_recv()
    routed = jnp.sum(rf[...].astype(F32), axis=0).reshape(16, 128)
    for k in range(4):
        out_ref[:, 128 * k : 128 * k + 128] = (own_rows[k] + routed[4 * k : 4 * k + 4]).astype(BF16)

    for ref, phase in (
        (rn.at[1:8], 0),
        (wq_r.at[0], 1),
        (wq_r.at[0], 12),
        (rh.at[1:4], 2),
        (rr.at[1:NZ], 3),
        (wo_r.at[0:2], 4),
        (rq.at[1:8], 5),
        (ro.at[1:NZ], 6),
        (wo_g.at[1:NSHORT], 7),
        (rd.at[1:NZ], 8),
        (rx.at[0, 1:NSHORT], 9),
        (re.at[0, 1:NSHORT], 10),
        (rf.at[1:NZ], 11),
        (rx.at[1, 1:NSHORT], 13),
        (re.at[1, 1:NSHORT], 14),
        (wq_g.at[1:NXC], 15),
        (wo_r.at[0:1], 16),
    ):
        all_of(ref, phase).wait_send()


def body(
    hidden,
    attn_gain,
    query_weight,
    head_bias,
    key_cache,
    value_cache,
    lengths,
    out_weight,
    moe_gain,
    route_group,
    route_inner,
    route_weight,
    gate_w,
    up_w,
    down_w,
):
    vmem = pl.BlockSpec(memory_space=pltpu.VMEM)
    hbm = pl.BlockSpec(memory_space=pltpu.HBM)

    def buf(*shape):
        return pltpu.VMEM(shape, BF16)

    return pl.pallas_call(
        kernel,
        out_shape=jax.ShapeDtypeStruct((4, 512), BF16),
        in_specs=[hbm] * 15,
        out_specs=vmem,
        scratch_shapes=[
            buf(4, 2048),
            pltpu.VMEM((16, 128), F32),
            buf(16, 512),
            pltpu.SMEM((16,), F32),
            pltpu.SMEM((4,), jnp.int32),
            buf(16, 512),
            pltpu.VMEM((16, 128), F32),
            pltpu.SMEM((4,), jnp.int32),
            pltpu.SMEM((2, 4), jnp.int32),
            buf(2, 4),
            buf(4, 1024, 128),
            buf(4, 1024, 128),
            buf(192, 2048),
            buf(192, 2048),
            buf(192, 2048),
            buf(2, 16, 512),
            buf(NXC, 2, 16, 512),
            buf(4, 16, 512),
            buf(NSHORT, 16, 512),
            buf(NZ, 8, 128),
            buf(8, 8, 128),
            buf(NZ, 8, 128),
            buf(8, 128),
            buf(8, 8, 128),
            buf(4, 8, 128),
            buf(NZ, 8, 128),
            buf(8, 2, 8, 128),
            buf(8, 2, 8, 128),
            buf(16, 128),
            buf(NZ, 16, 128),
            buf(16, 128),
            buf(NZ, 16, 128),
            buf(NXC, 2, 4, 8, 128),
            buf(2, NSHORT, 4, 8, 128),
            buf(2, NXC, NY, 4, 8, 128),
            buf(2, NSHORT, 4, 8, 128),
            buf(2, 8, 2, 8, 128),
            buf(NZ, 2, 8, 128),
            pltpu.SemaphoreType.DMA((15,)),
            pltpu.SemaphoreType.DMA((17,)),
            pltpu.SemaphoreType.DMA((17,)),
        ],
        compiler_params=pltpu.CompilerParams(
            collective_id=0, has_side_effects=True, vmem_limit_bytes=67043328
        ),
        name="layer",
    )(
        hidden,
        attn_gain.reshape(16, 128),
        query_weight,
        head_bias,
        key_cache.reshape(4, 1024, 128),
        value_cache.reshape(4, 1024, 128),
        lengths,
        out_weight.T,
        moe_gain.reshape(16, 128),
        route_group,
        route_inner.T,
        route_weight.T,
        jnp.swapaxes(gate_w, 1, 2).reshape(192, 2048),
        jnp.swapaxes(up_w, 1, 2).reshape(192, 2048),
        down_w.reshape(192, 2048),
    )


def solution(mesh):
    torus = Mesh(mesh.devices.reshape(NZ, NX, NC, NY), ("ep_0", "ep_1", "ep_2", "tp"))
    placed = (
        P(EP, None),
        P(),
        P(EP, "tp"),
        P(),
        P(EP, "tp", None, None),
        P(EP, "tp", None, None),
        P(EP),
        P("tp", EP),
        P(),
        P(EP),
        P(EP, None),
        P(EP, None),
        P(EP, None, "tp"),
        P(EP, None, "tp"),
        P(EP, "tp", None),
    )
    return jax.shard_map(body, mesh=torus, in_specs=placed, out_specs=P(EP, "tp"), check_vma=False)
```

```python
import jax
import jax.numpy as jnp
from jax import lax
from jax.experimental import pallas as pl
from jax.experimental.pallas import tpu as pltpu
from jax.sharding import Mesh
from jax.sharding import PartitionSpec as P

EP = ("ep_0", "ep_1", "ep_2")
MESH = pl.DeviceIdType.MESH
F32 = jnp.float32
BF16 = jnp.bfloat16
NZ, NX, NC, NY = 16, 4, 2, 4
NXC = NX * NC
NSHORT = NXC * NY
EPS = 1e-06

Z_ORDER = (8, 7, 9, 6, 10, 5, 11, 4, 12, 3, 13, 2, 14, 1, 15)
NEAR_ORDER = (4, 12, 3, 13, 2, 14, 1, 15)
HOPS = (0, 1, 2, 1)
XC_ORDER = sorted(((dx, dc) for dx in range(NX) for dc in range(NC) if dx or dc), key=lambda d: (-HOPS[d[0]], d))
SHORT_ORDER = sorted(
    ((dx, dc, dy) for dx in range(NX) for dc in range(NC) for dy in range(NY) if dx or dc or dy),
    key=lambda d: (-HOPS[d[0]] - HOPS[d[2]], d),
)

NT = (((1,), (1,)), ((), ()))
TN = (((0,), (0,)), ((), ()))


def dot(a, b, dims=None, precision=None):
    if dims is None:
        dims = (((1,), (0,)), ((), ()))
    return lax.dot_general(a, b, dims, precision=precision, preferred_element_type=F32)


def iota(shape, dim):
    return lax.broadcasted_iota(jnp.int32, shape, dim)


def kernel(
    hid_hbm,
    again_hbm,
    wq_hbm,
    bias_hbm,
    k_hbm,
    v_hbm,
    len_hbm,
    wo_hbm,
    mgain_hbm,
    rg_hbm,
    ri_hbm,
    rw_hbm,
    gate_hbm,
    up_hbm,
    down_hbm,
    out_ref,
    hid_ref,
    again_ref,
    wq_ref,
    bias_ref,
    len_ref,
    wo_t,
    mgain_ref,
    rg_ref,
    ri_ref,
    rw_ref,
    k_v,
    v_v,
    wg_v,
    wu_v,
    wd_v,
    wq_r,
    wq_g,
    wo_r,
    wo_g,
    sn,
    st,
    sh,
    sr,
    rn,
    rh,
    rr,
    sq,
    rq,
    so,
    ro,
    sd,
    rd,
    sx4,
    rx4,
    se4,
    re4,
    sx,
    rx,
    se,
    re,
    sf,
    rf,
    load_sem,
    send_sem,
    recv_sem,
    past_sem,
):
    z = lax.axis_index("ep_0")
    x = lax.axis_index("ep_1")
    c = lax.axis_index("ep_2")
    y = lax.axis_index("tp")
    xc = x * NC + c
    me = xc * NY + y

    def z_at(off):
        return lax.rem(z + off, NZ)

    def xc_at(dx, dc):
        return lax.rem(x + dx, NX), lax.rem(c + dc, NC)

    def y_at(dy):
        return lax.rem(y + dy, NY)

    barrier = pltpu.get_barrier_semaphore()

    def greet(device):
        pl.semaphore_signal(barrier, inc=1, device_id=device, device_id_type=MESH)

    for off in NEAR_ORDER:
        greet((z_at(off), x, c, y))
    for dx, dc in XC_ORDER:
        greet((z, *xc_at(dx, dc), y))
    for dy in range(1, NY):
        greet((z, x, c, y_at(dy)))
    greeted = len(NEAR_ORDER) + NXC - 1 + NY - 1

    copies = (
        (hid_hbm, hid_ref),
        (again_hbm, again_ref),
        (rw_hbm, rw_ref),
        (rg_hbm, rg_ref),
        (ri_hbm, ri_ref),
        (wq_hbm, wq_ref),
        (wo_hbm, wo_t),
        (bias_hbm, bias_ref),
        (len_hbm, len_ref),
        (mgain_hbm, mgain_ref),
        (k_hbm, k_v),
        (v_hbm, v_v),
        (gate_hbm, wg_v),
        (up_hbm, wu_v),
        (down_hbm, wd_v),
    )
    loads = [pltpu.make_async_copy(src, dst, load_sem.at[i]) for i, (src, dst) in enumerate(copies)]
    for one in loads:
        one.start()
    for one in loads[0:5]:
        one.wait()

    hid = hid_ref[...].astype(F32)
    scale = lax.rsqrt(jnp.mean(hid * hid, axis=-1, keepdims=True) + EPS)
    hid2 = jnp.concatenate([hid, hid], axis=0)
    scale2 = jnp.concatenate([scale, scale], axis=0)
    for k in range(NZ):
        part = hid2[:, 128 * k : 128 * k + 128]
        sn[k] = (part * scale2 * again_ref[k : k + 1, :]).astype(BF16)
        sh[k] = part.astype(BF16)
    first8 = iota((8, 128), 0) < 4
    for i in range(8):
        st[i] = jnp.where(first8, sn[z_at(i)].astype(F32), sn[z_at(i + 8)].astype(F32)).astype(BF16)

    lane = iota((1, 128), 1)
    tok_a = lane % 4
    near = (lane % 64) // 4 == z
    wide = lane // 8 == z
    route_w = rw_ref[...].astype(F32)
    rows = []
    for pattern in (near, wide):
        for k in range(2):
            row = jnp.zeros((1, 128), F32)
            for t in range(4):
                ident = (rg_ref[t] * 32 + ri_ref[k, t]).astype(F32)
                row = jnp.where(tok_a == t, ident, row)
            rows.append(jnp.where(pattern, row, 0.0))
    for k in range(2):
        row = jnp.zeros((1, 128), F32)
        for t in range(4):
            row = jnp.where(tok_a == t, route_w[k : k + 1, t : t + 1], row)
        rows.append(jnp.where(wide, row, 0.0))
    rowid = iota((8, 128), 0)
    packet = jnp.zeros((8, 128), F32)
    for k, row in enumerate(rows):
        packet = jnp.where(rowid == k, jnp.broadcast_to(row, (8, 128)), packet)
    sr[...] = packet.astype(BF16)

    for one in loads[5:10]:
        one.wait()
    pl.semaphore_wait(barrier, greeted)

    def send(device, src, dst, phase):
        pltpu.make_async_remote_copy(
            src_ref=src,
            dst_ref=dst,
            send_sem=send_sem.at[phase],
            recv_sem=recv_sem.at[phase],
            device_id=device,
            device_id_type=MESH,
        ).start()

    def all_of(ref, phase):
        return pltpu.make_async_remote_copy(
            src_ref=ref,
            dst_ref=ref,
            send_sem=send_sem.at[phase],
            recv_sem=recv_sem.at[phase],
            device_id=(z_at(1), x, c, y),
            device_id_type=MESH,
        )

    quad = lax.div(z, 4)

    def share(slot):
        source = wo_r.at[slot] if slot else wo_t
        p = lax.rem(quad + slot, NY)
        for dx, dc in XC_ORDER:
            send((z, *xc_at(dx, dc), p), source, wo_g.at[y * NXC + xc], 7)

        @pl.when(p != y)
        def _():
            send((z, x, c, p), source, wo_g.at[y * NXC + xc], 7)

        @pl.when(p == y)
        def _():
            wo_g[y * NXC + xc] = source[...]

    send((z_at(12), x, c, y), wq_ref, wq_r.at[0], 1)
    send((z_at(4), x, c, y), wq_ref, wq_r.at[1], 12)
    for i in (0, 1, 7, 2, 6, 3, 5):
        send((z_at((i - 4) % NZ), x, c, y), st.at[i], rn.at[i], 0)
    for slot, off in ((1, 12), (3, 4)):
        send((z_at(off), x, c, y), wo_t, wo_r.at[slot], 4)

    def near_chunk(off):
        return lax.rem(z + off, 4) + 4 * y

    for i in range(4):
        if i != 2:
            off = (2 - i) % NZ
            send((z_at(off), x, c, y), sh.at[near_chunk(off)], rh.at[i], 2)
    rn[4] = st[4]
    rr[0] = sr[...]
    rh[2] = sh[near_chunk(0)]
    for dx, dc in XC_ORDER:
        pl.semaphore_signal(past_sem, inc=1, device_id=(z, *xc_at(dx, dc), y), device_id_type=MESH)

    def gather_rows(slot, phase):
        all_of(wq_r.at[0], phase).wait_recv()
        for dx, dc in XC_ORDER:
            send((z, *xc_at(dx, dc), y), wq_r.at[slot], wq_g.at[xc, slot], 15)

    @pl.when(lax.rem(quad, 2) == 0)
    def _():
        gather_rows(0, 1)
        gather_rows(1, 12)

    @pl.when(lax.rem(quad, 2) == 1)
    def _():
        gather_rows(1, 12)
        gather_rows(0, 1)

    wq_g[xc] = wq_r[...]
    all_of(wo_r.at[0:2], 4).wait_recv()
    send((z_at(12), x, c, y), wo_r.at[1], wo_r.at[2], 16)
    for off in Z_ORDER:
        send((z_at(off), x, c, y), sr, rr.at[NZ - off], 3)
    pl.semaphore_wait(past_sem, NXC - 1)
    for slot in (0, 1, 3):
        share(slot)
    all_of(rn.at[1:8], 0).wait_recv()
    xin = rn[...].astype(F32).reshape(64, 128).astype(BF16)
    all_of(wq_g.at[1:NXC], 15).wait_recv()

    first_q = (iota((64, 512), 0) % 8) < 4
    part_q = jnp.where(
        first_q, dot(xin, wq_g[:, 0].reshape(128, 512)), dot(xin, wq_g[:, 1].reshape(128, 512))
    ).reshape(8, 8, 512)
    part_q = (part_q + pltpu.roll(part_q, 4, 1)).reshape(64, 512)
    first = first_q[:, 0:128]
    for p in range(2):
        pair = jnp.where(first, part_q[:, 256 * p : 256 * p + 128], part_q[:, 256 * p + 128 : 256 * p + 256])
        sq[:, p] = pair.reshape(8, 8, 128).astype(BF16)
    for i in (0, 1, 7, 2, 6, 3, 5):
        send((z_at((4 - i) % NZ), x, c, y), sq.at[i], rq.at[i], 5)
    rq[4] = sq[4]


    later = (iota((128, 128), 0) > iota((128, 128), 1)).astype(F32)
    rowh = iota((16, 1), 0)
    bias = jnp.zeros((16, 1), F32)
    length = jnp.zeros((16, 1), jnp.int32)
    for h in range(4):
        bias = jnp.where(rowh // 4 == h, bias_ref[4 * y + h], bias)
        length = jnp.where(rowh % 4 == h, len_ref[h], length)

    all_of(wo_r.at[0:1], 16).wait_recv()
    share(2)
    all_of(rq.at[1:8], 5).wait_recv()
    q = jnp.sum(rq[...].astype(F32), axis=0).reshape(16, 128).astype(BF16)
    loads[10].wait()
    tok = iota((16, 1024), 0) % 4
    scores = jnp.zeros((16, 1024), F32)
    for t in range(4):
        scores = jnp.where(tok == t, dot(q, k_v[t], NT), scores)
    scores = scores * (128.0 ** -0.5) + bias
    soft = jnp.log1p(jnp.exp(-jnp.abs(scores)))
    log_stop = jnp.minimum(scores, 0.0) - soft
    visible = iota((16, 1024), 1) < length
    log_keep = jnp.where(visible, log_stop - scores, 0.0)
    stacked = jnp.concatenate([log_keep[:, 128 * k : 128 * k + 128] for k in range(8)], axis=0)
    within = dot(stacked, later, precision=lax.Precision.HIGHEST)
    carry_sum = jnp.zeros((16, 1), F32)
    weights = [None] * 8
    for k in reversed(range(8)):
        inner = within[16 * k : 16 * k + 16]
        keep_k = log_keep[:, 128 * k : 128 * k + 128]
        expo = jnp.exp(log_stop[:, 128 * k : 128 * k + 128] + (inner + carry_sum))
        weights[k] = jnp.where(visible[:, 128 * k : 128 * k + 128], expo, 0.0)
        carry_sum = carry_sum + (inner[:, 0:1] + keep_k[:, 0:1])
    weight = jnp.concatenate(weights, axis=1).astype(BF16)
    loads[11].wait()
    tok_o = iota((16, 128), 0) % 4
    heads = jnp.zeros((16, 128), F32)
    for t in range(4):
        heads = jnp.where(tok_o == t, dot(weight, v_v[t]), heads)
    so[...] = heads.astype(BF16)

    for dy in (2, 1, 3, 0):
        for i in (0, 1, 3, 2):
            if dy or i != 2:
                send((z_at((2 - i) % NZ), x, c, y_at(dy)), so, ro.at[4 * y + i], 6)
    ro[4 * y + 2] = so[...]

    all_of(rh.at[1:4], 2).wait_recv()
    all_of(wo_g.at[1:NSHORT], 7).wait_recv()
    all_of(ro.at[1:NZ], 6).wait_recv()
    head_row = (iota((64, 128), 0) % 16) // 4
    resid = rh[...].astype(F32)
    for p in range(NY):
        heads_in = ro[4 * p : 4 * p + 4].reshape(64, 128)
        wo_p = wo_g[NXC * p : NXC * p + NXC].reshape(128, 512)
        proj = jnp.zeros((64, 128), F32)
        for h in range(4):
            proj = jnp.where(head_row == h, dot(heads_in, wo_p[:, 128 * h : 128 * h + 128], NT), proj)
        proj = jnp.sum(proj.reshape(4, 2, 8, 128), axis=1)
        proj = proj + pltpu.roll(proj, 4, 1)
        resid = resid + proj.astype(BF16).astype(F32)
    sd[...] = jnp.concatenate(
        [jnp.where(first8, resid[0], resid[1]), jnp.where(first8, resid[2], resid[3])], axis=0
    ).astype(BF16)

    for off in Z_ORDER:
        send((z_at(off), x, c, y), sd, rd.at[z], 8)
    rd[z] = sd[...]

    all_of(rr.at[1:NZ], 3).wait_recv()
    route = jnp.sum(rr[...].astype(F32), axis=0)

    groups = ((0, 4), (4, 4), (8, 8))

    def select_of(start, count, base, size):
        shape = (64, 16 * count)
        row = iota(shape, 0)
        expert = (NXC * z + row // 8).astype(F32)
        same = iota(shape, 1) // 4 + (start - 2) == base + row % size
        own = pltpu.roll(route, (4 * (2 - start)) % 128, 1)
        wanted = (own[0:1, 0 : 16 * count] == expert) | (own[1:2, 0 : 16 * count] == expert)
        return jnp.where(same & wanted, 1.0, 0.0).astype(BF16)

    def holders(base, size):
        counts = (3, 3, 2, 3) if size == 8 else (2, 2, 1, 2)
        return tuple((base + off, count) for off, count in zip((0, 1, 2, -1), counts))

    selects = [[select_of(*one, base, size) for one in holders(base, size)] for base, size in groups]

    def combine_of(base, size):
        rows, cols = (128, 64) if size == 8 else (64, 32)
        row = iota((rows, cols), 0)
        col = iota((rows, cols), 1)
        own = route[:, 8 * base : 8 * base + cols]
        if size == 8:
            expert, chunk, block = (row // 8) % NXC, row // 64, row % 8
        else:
            expert, chunk, block = row // 8, (row // 4) % 2, row % 4
        expert = (NXC * z + expert).astype(F32)
        same = (block == col // 8) & (chunk == (col // 4) % 2)
        weight = jnp.where(own[2:3] == expert, own[4:5], 0.0) + jnp.where(own[3:4] == expert, own[5:6], 0.0)
        return jnp.where(same, weight, 0.0).astype(BF16)

    combines = [combine_of(base, size) for base, size in groups]
    first64 = (iota((64, 128), 0) % 8) < 4
    first_ff = (iota((64, 192), 0) % 8) < 4
    bufs = ((sx4.at[0], rx4.at[0], se4.at[0], re4.at[0]), (sx4.at[1], rx4.at[1], se4.at[1], re4.at[1]), (sx, rx, se, re))

    def swap(v):
        return pltpu.roll(v.reshape(8, 8, v.shape[1]), 4, 1).reshape(v.shape)

    def to_experts(n, phase):
        out, into = bufs[n][0], bufs[n][1]
        base, size = groups[n]
        slots = []
        for k, (start, count) in enumerate(holders(base, size)):
            rows = jnp.concatenate([rd[(start + 4 * i) % NZ] for i in range(count)], axis=0)
            slots.append(dot(selects[n][k], rows))
        if size == 4:
            slots = [jnp.where(first64, slots[0], slots[1]), jnp.where(first64, slots[2], slots[3])]
        for k, slot in enumerate(slots):
            out[:, k] = slot.reshape(NXC, 8, 128).astype(BF16)
        for dx, dc, dy in SHORT_ORDER:
            px, pc = xc_at(dx, dc)
            send((z, px, pc, y_at(dy)), out.at[px * NC + pc], into.at[me], phase)
        into[me] = out[xc]

    all_of(rd.at[1:NZ], 8).wait_recv()
    to_experts(0, 9)
    to_experts(1, 17)
    to_experts(2, 13)

    pieces = [rd[z_at(18 - i)].astype(F32)[4 * i : 4 * i + 4] for i in range(4)]
    own_rows = []
    for k in range(4):
        row = jnp.zeros((4, 128), F32)
        for i in range(4):
            row = jnp.where(lax.rem(z + 18 - i, 4) == k, pieces[i], row)
        own_rows.append(row)

    def experts(n, phase):
        _, into, out, back = bufs[n]
        small = groups[n][1] == 4
        tiles = 2 if small else 4
        slots = into.reshape(NXC, NY, tiles, 8, 128)
        chunks = [slots[:, k // tiles, k % tiles].astype(F32).reshape(64, 128) for k in range(NY * tiles)]
        square = chunks[0] * chunks[0]
        for chunk in chunks[1:]:
            square = square + chunk * chunk
        if small:
            square = square + swap(square)
        scale_two = lax.rsqrt(jnp.sum(square, axis=-1, keepdims=True) * (1.0 / 2048.0) + EPS)

        def gain(k):
            if small:
                return jnp.where(first64, mgain_ref[2 * k : 2 * k + 1, :], mgain_ref[2 * k + 1 : 2 * k + 2, :])
            return mgain_ref[k : k + 1, :]

        lhs = jnp.concatenate([(one * scale_two * gain(k)).astype(BF16) for k, one in enumerate(chunks)], axis=1)

        def product(w):
            if not small:
                return dot(lhs, w[...], NT)
            even, odd = [
                dot(lhs, jnp.concatenate([w[:, 256 * k + o : 256 * k + o + 128] for k in range(8)], axis=1), NT)
                for o in (0, 128)
            ]
            both = jnp.where(first_ff, even, odd)
            return both + swap(both)

        gated = product(wg_v)
        upped = product(wu_v)
        act = (gated / (1.0 + jnp.exp(-gated)) * upped).astype(BF16)
        for p in range(NY):
            down = dot(act, wd_v[:, 512 * p : 512 * p + 512])
            parts = [down[:, 128 * k : 128 * k + 128] for k in range(4)]
            if small:
                parts = [jnp.where(first64, parts[0], parts[1]), jnp.where(first64, parts[2], parts[3])]
            for k, part in enumerate(parts):
                out[:, p, k] = part.reshape(NXC, 8, 128).astype(BF16)
        for dx, dc, dy in SHORT_ORDER:
            px, pc = xc_at(dx, dc)
            p = y_at(dy)
            send((z, px, pc, p), out.at[px * NC + pc, p], back.at[me], phase)
        back[me] = out[xc, y]

    def to_tokens(n):
        base, size = groups[n]
        tiles = 2 if size == 4 else 4
        parts = bufs[n][3].reshape(NXC, NY, tiles, 8, 128)
        totals = []
        for k in range(tiles):
            total = parts[:, 0, k].astype(F32)
            for p in range(1, NY):
                total = total + parts[:, p, k].astype(F32)
            totals.append(total.reshape(64, 128).astype(BF16))
        if size == 8:
            totals = [jnp.concatenate(totals[2 * p : 2 * p + 2], axis=0) for p in range(2)]
        for p in range(2):
            sf[base : base + size, p] = dot(combines[n], totals[p], TN).reshape(size, 8, 128).astype(BF16)

        def back(j):
            b = base + lax.rem(z + j, size)
            send((b, x, c, y), sf.at[b], rf.at[z], 11)

        @pl.when(lax.div(z, size) != base // size)
        def _():
            back(0)

        for j in range(1, size):
            back(j)

    for one in loads[12:]:
        one.wait()
    all_of(rx4.at[0, 1:NSHORT], 9).wait_recv()
    experts(0, 10)
    all_of(rx4.at[1, 1:NSHORT], 17).wait_recv()
    experts(1, 18)
    all_of(rx.at[1:NSHORT], 13).wait_recv()
    experts(2, 14)
    all_of(re4.at[0, 1:NSHORT], 10).wait_recv()
    to_tokens(0)
    all_of(re4.at[1, 1:NSHORT], 18).wait_recv()
    to_tokens(1)
    all_of(re.at[1:NSHORT], 14).wait_recv()
    to_tokens(2)
    rf[z] = sf[z]

    all_of(rf.at[1:NZ], 11).wait_recv()
    routed = jnp.sum(rf[...].astype(F32), axis=0).reshape(16, 128)
    for k in range(4):
        out_ref[:, 128 * k : 128 * k + 128] = (own_rows[k] + routed[4 * k : 4 * k + 4]).astype(BF16)

    for ref, phase in (
        (rn.at[1:8], 0),
        (wq_r.at[0], 1),
        (wq_r.at[0], 12),
        (rh.at[1:4], 2),
        (rr.at[1:NZ], 3),
        (wo_r.at[0:2], 4),
        (rq.at[1:8], 5),
        (ro.at[1:NZ], 6),
        (wo_g.at[1:NSHORT], 7),
        (rd.at[1:NZ], 8),
        (rx4.at[0, 1:NSHORT], 9),
        (rx4.at[1, 1:NSHORT], 17),
        (re4.at[1, 1:NSHORT], 18),
        (re4.at[0, 1:NSHORT], 10),
        (rf.at[1:NZ], 11),
        (rx.at[1:NSHORT], 13),
        (re.at[1:NSHORT], 14),
        (wq_g.at[1:NXC], 15),
        (wo_r.at[0:1], 16),
    ):
        all_of(ref, phase).wait_send()


def body(
    hidden,
    attn_gain,
    query_weight,
    head_bias,
    key_cache,
    value_cache,
    lengths,
    out_weight,
    moe_gain,
    route_group,
    route_inner,
    route_weight,
    gate_w,
    up_w,
    down_w,
):
    vmem = pl.BlockSpec(memory_space=pltpu.VMEM)
    hbm = pl.BlockSpec(memory_space=pltpu.HBM)

    def buf(*shape):
        return pltpu.VMEM(shape, BF16)

    return pl.pallas_call(
        kernel,
        out_shape=jax.ShapeDtypeStruct((4, 512), BF16),
        in_specs=[hbm] * 15,
        out_specs=vmem,
        scratch_shapes=[
            buf(4, 2048),
            pltpu.VMEM((16, 128), F32),
            buf(16, 512),
            pltpu.SMEM((16,), F32),
            pltpu.SMEM((4,), jnp.int32),
            buf(16, 512),
            pltpu.VMEM((16, 128), F32),
            pltpu.SMEM((4,), jnp.int32),
            pltpu.SMEM((2, 4), jnp.int32),
            buf(2, 4),
            buf(4, 1024, 128),
            buf(4, 1024, 128),
            buf(192, 2048),
            buf(192, 2048),
            buf(192, 2048),
            buf(2, 16, 512),
            buf(NXC, 2, 16, 512),
            buf(4, 16, 512),
            buf(NSHORT, 16, 512),
            buf(NZ, 8, 128),
            buf(8, 8, 128),
            buf(NZ, 8, 128),
            buf(8, 128),
            buf(8, 8, 128),
            buf(4, 8, 128),
            buf(NZ, 8, 128),
            buf(8, 2, 8, 128),
            buf(8, 2, 8, 128),
            buf(16, 128),
            buf(NZ, 16, 128),
            buf(16, 128),
            buf(NZ, 16, 128),
            buf(2, NXC, 2, 8, 128),
            buf(2, NSHORT, 2, 8, 128),
            buf(2, NXC, NY, 2, 8, 128),
            buf(2, NSHORT, 2, 8, 128),
            buf(NXC, 4, 8, 128),
            buf(NSHORT, 4, 8, 128),
            buf(NXC, NY, 4, 8, 128),
            buf(NSHORT, 4, 8, 128),
            buf(NZ, 2, 8, 128),
            buf(NZ, 2, 8, 128),
            pltpu.SemaphoreType.DMA((15,)),
            pltpu.SemaphoreType.DMA((19,)),
            pltpu.SemaphoreType.DMA((19,)),
            pltpu.SemaphoreType.REGULAR,
        ],
        compiler_params=pltpu.CompilerParams(
            collective_id=0, has_side_effects=True, vmem_limit_bytes=67043328
        ),
        name="layer",
    )(
        hidden,
        attn_gain.reshape(16, 128),
        query_weight,
        head_bias,
        key_cache.reshape(4, 1024, 128),
        value_cache.reshape(4, 1024, 128),
        lengths,
        out_weight.T,
        moe_gain.reshape(16, 128),
        route_group,
        route_inner.T,
        route_weight.T,
        jnp.swapaxes(gate_w, 1, 2).reshape(192, 2048),
        jnp.swapaxes(up_w, 1, 2).reshape(192, 2048),
        down_w.reshape(192, 2048),
    )


def solution(mesh):
    torus = Mesh(mesh.devices.reshape(NZ, NX, NC, NY), ("ep_0", "ep_1", "ep_2", "tp"))
    placed = (
        P(EP, None),
        P(),
        P(EP, "tp"),
        P(),
        P(EP, "tp", None, None),
        P(EP, "tp", None, None),
        P(EP),
        P("tp", EP),
        P(),
        P(EP),
        P(EP, None),
        P(EP, None),
        P(EP, None, "tp"),
        P(EP, None, "tp"),
        P(EP, "tp", None),
    )
    return jax.shard_map(body, mesh=torus, in_specs=placed, out_specs=P(EP, "tp"), check_vma=False)
```

```python
import jax
import jax.numpy as jnp
from jax import lax
from jax.experimental import pallas as pl
from jax.experimental.pallas import tpu as pltpu
from jax.sharding import Mesh
from jax.sharding import PartitionSpec as P

EP = ("ep_0", "ep_1", "ep_2")
MESH = pl.DeviceIdType.MESH
F32 = jnp.float32
BF16 = jnp.bfloat16
NZ, NX, NC, NY = 16, 4, 2, 4
NXC = NX * NC
NSHORT = NXC * NY
EPS = 1e-06

Z_ORDER = (8, 7, 9, 6, 10, 5, 11, 4, 12, 3, 13, 2, 14, 1, 15)
NEAR_ORDER = (4, 12, 3, 13, 2, 14, 1, 15)
HOPS = (0, 1, 2, 1)
XC_ORDER = sorted(((dx, dc) for dx in range(NX) for dc in range(NC) if dx or dc), key=lambda d: (-HOPS[d[0]], d))
SHORT_ORDER = sorted(
    ((dx, dc, dy) for dx in range(NX) for dc in range(NC) for dy in range(NY) if dx or dc or dy),
    key=lambda d: (-HOPS[d[0]] - HOPS[d[2]], d),
)

NT = (((1,), (1,)), ((), ()))
TN = (((0,), (0,)), ((), ()))


def dot(a, b, dims=None, precision=None):
    if dims is None:
        dims = (((1,), (0,)), ((), ()))
    return lax.dot_general(a, b, dims, precision=precision, preferred_element_type=F32)


def iota(shape, dim):
    return lax.broadcasted_iota(jnp.int32, shape, dim)


def kernel(
    hid_hbm,
    again_hbm,
    wq_hbm,
    bias_hbm,
    k_hbm,
    v_hbm,
    len_hbm,
    wo_hbm,
    mgain_hbm,
    rg_hbm,
    ri_hbm,
    rw_hbm,
    gate_hbm,
    up_hbm,
    down_hbm,
    out_ref,
    hid_ref,
    again_ref,
    wq_ref,
    bias_ref,
    len_ref,
    wo_t,
    mgain_ref,
    rg_ref,
    ri_ref,
    rw_ref,
    k_v,
    v_v,
    wg_v,
    wu_v,
    wd_v,
    wq_r,
    wq_g,
    wo_r,
    wo_g,
    sn,
    st,
    sh,
    sr,
    rn,
    rh,
    rr,
    sq,
    rq,
    so,
    ro,
    sd,
    rd,
    sx4,
    rx4,
    se4,
    re4,
    sx,
    rx,
    se,
    re,
    sf,
    rf,
    load_sem,
    send_sem,
    recv_sem,
    past_sem,
):
    z = lax.axis_index("ep_0")
    x = lax.axis_index("ep_1")
    c = lax.axis_index("ep_2")
    y = lax.axis_index("tp")
    xc = x * NC + c
    me = xc * NY + y

    def z_at(off):
        return lax.rem(z + off, NZ)

    def xc_at(dx, dc):
        return lax.rem(x + dx, NX), lax.rem(c + dc, NC)

    def y_at(dy):
        return lax.rem(y + dy, NY)

    barrier = pltpu.get_barrier_semaphore()

    def greet(device):
        pl.semaphore_signal(barrier, inc=1, device_id=device, device_id_type=MESH)

    for off in NEAR_ORDER:
        greet((z_at(off), x, c, y))
    for dx, dc in XC_ORDER:
        greet((z, *xc_at(dx, dc), y))
    for dy in range(1, NY):
        greet((z, x, c, y_at(dy)))
    greeted = len(NEAR_ORDER) + NXC - 1 + NY - 1

    copies = (
        (hid_hbm, hid_ref),
        (again_hbm, again_ref),
        (rw_hbm, rw_ref),
        (rg_hbm, rg_ref),
        (ri_hbm, ri_ref),
        (wq_hbm, wq_ref),
        (wo_hbm, wo_t),
        (bias_hbm, bias_ref),
        (len_hbm, len_ref),
        (mgain_hbm, mgain_ref),
        (k_hbm, k_v),
        (v_hbm, v_v),
        (gate_hbm, wg_v),
        (up_hbm, wu_v),
        (down_hbm, wd_v),
    )
    loads = [pltpu.make_async_copy(src, dst, load_sem.at[i]) for i, (src, dst) in enumerate(copies)]
    for one in loads:
        one.start()
    for one in loads[0:5]:
        one.wait()

    hid = hid_ref[...].astype(F32)
    scale = lax.rsqrt(jnp.mean(hid * hid, axis=-1, keepdims=True) + EPS)
    hid2 = jnp.concatenate([hid, hid], axis=0)
    scale2 = jnp.concatenate([scale, scale], axis=0)
    for k in range(NZ):
        part = hid2[:, 128 * k : 128 * k + 128]
        sn[k] = (part * scale2 * again_ref[k : k + 1, :]).astype(BF16)
        sh[k] = part.astype(BF16)
    first8 = iota((8, 128), 0) < 4
    for i in range(8):
        st[i] = jnp.where(first8, sn[z_at(i)].astype(F32), sn[z_at(i + 8)].astype(F32)).astype(BF16)

    lane = iota((1, 128), 1)
    tok_a = lane % 4
    near = (lane % 64) // 4 == z
    wide = lane // 8 == z
    route_w = rw_ref[...].astype(F32)
    rows = []
    for pattern in (near, wide):
        for k in range(2):
            row = jnp.zeros((1, 128), F32)
            for t in range(4):
                ident = (rg_ref[t] * 32 + ri_ref[k, t]).astype(F32)
                row = jnp.where(tok_a == t, ident, row)
            rows.append(jnp.where(pattern, row, 0.0))
    for k in range(2):
        row = jnp.zeros((1, 128), F32)
        for t in range(4):
            row = jnp.where(tok_a == t, route_w[k : k + 1, t : t + 1], row)
        rows.append(jnp.where(wide, row, 0.0))
    rowid = iota((8, 128), 0)
    packet = jnp.zeros((8, 128), F32)
    for k, row in enumerate(rows):
        packet = jnp.where(rowid == k, jnp.broadcast_to(row, (8, 128)), packet)
    sr[...] = packet.astype(BF16)

    for one in loads[5:10]:
        one.wait()
    pl.semaphore_wait(barrier, greeted)

    def send(device, src, dst, phase):
        pltpu.make_async_remote_copy(
            src_ref=src,
            dst_ref=dst,
            send_sem=send_sem.at[phase],
            recv_sem=recv_sem.at[phase],
            device_id=device,
            device_id_type=MESH,
        ).start()

    def all_of(ref, phase):
        return pltpu.make_async_remote_copy(
            src_ref=ref,
            dst_ref=ref,
            send_sem=send_sem.at[phase],
            recv_sem=recv_sem.at[phase],
            device_id=(z_at(1), x, c, y),
            device_id_type=MESH,
        )

    quad = lax.div(z, 4)

    def share(slot):
        source = wo_r.at[slot] if slot else wo_t
        p = lax.rem(quad + slot, NY)
        for dx, dc in XC_ORDER:
            send((z, *xc_at(dx, dc), p), source, wo_g.at[y * NXC + xc], 7)

        @pl.when(p != y)
        def _():
            send((z, x, c, p), source, wo_g.at[y * NXC + xc], 7)

        @pl.when(p == y)
        def _():
            wo_g[y * NXC + xc] = source[...]

    send((z_at(12), x, c, y), wq_ref, wq_r.at[0], 1)
    send((z_at(4), x, c, y), wq_ref, wq_r.at[1], 12)
    for i in (0, 1, 7, 2, 6, 3, 5):
        send((z_at((i - 4) % NZ), x, c, y), st.at[i], rn.at[i], 0)
    for slot, off in ((1, 12), (3, 4)):
        send((z_at(off), x, c, y), wo_t, wo_r.at[slot], 4)

    def near_chunk(off):
        return lax.rem(z + off, 4) + 4 * y

    for i in range(4):
        if i != 2:
            off = (2 - i) % NZ
            send((z_at(off), x, c, y), sh.at[near_chunk(off)], rh.at[i], 2)
    rn[4] = st[4]
    rr[0] = sr[...]
    rh[2] = sh[near_chunk(0)]
    for dx, dc in XC_ORDER:
        pl.semaphore_signal(past_sem, inc=1, device_id=(z, *xc_at(dx, dc), y), device_id_type=MESH)

    pl.semaphore_wait(past_sem, NXC - 1)
    share(0)
    def gather_rows(slot, phase):
        all_of(wq_r.at[0], phase).wait_recv()
        for dx, dc in XC_ORDER:
            send((z, *xc_at(dx, dc), y), wq_r.at[slot], wq_g.at[xc, slot], 15)

    @pl.when(lax.rem(quad, 2) == 0)
    def _():
        gather_rows(0, 1)
        gather_rows(1, 12)

    @pl.when(lax.rem(quad, 2) == 1)
    def _():
        gather_rows(1, 12)
        gather_rows(0, 1)

    wq_g[xc] = wq_r[...]
    all_of(wo_r.at[0:2], 4).wait_recv()
    send((z_at(12), x, c, y), wo_r.at[1], wo_r.at[2], 16)
    for off in Z_ORDER:
        send((z_at(off), x, c, y), sr, rr.at[NZ - off], 3)
    all_of(rn.at[1:8], 0).wait_recv()
    xin = rn[...].astype(F32).reshape(64, 128).astype(BF16)
    all_of(wq_g.at[1:NXC], 15).wait_recv()

    first_q = (iota((64, 512), 0) % 8) < 4
    part_q = jnp.where(
        first_q, dot(xin, wq_g[:, 0].reshape(128, 512)), dot(xin, wq_g[:, 1].reshape(128, 512))
    ).reshape(8, 8, 512)
    part_q = (part_q + pltpu.roll(part_q, 4, 1)).reshape(64, 512)
    first = first_q[:, 0:128]
    for p in range(2):
        pair = jnp.where(first, part_q[:, 256 * p : 256 * p + 128], part_q[:, 256 * p + 128 : 256 * p + 256])
        sq[:, p] = pair.reshape(8, 8, 128).astype(BF16)
    for i in (0, 1, 7, 2, 6, 3, 5):
        send((z_at((4 - i) % NZ), x, c, y), sq.at[i], rq.at[i], 5)
    rq[4] = sq[4]

    share(1)
    share(3)


    later = (iota((128, 128), 0) > iota((128, 128), 1)).astype(F32)
    rowh = iota((16, 1), 0)
    bias = jnp.zeros((16, 1), F32)
    length = jnp.zeros((16, 1), jnp.int32)
    for h in range(4):
        bias = jnp.where(rowh // 4 == h, bias_ref[4 * y + h], bias)
        length = jnp.where(rowh % 4 == h, len_ref[h], length)

    all_of(wo_r.at[0:1], 16).wait_recv()
    share(2)
    all_of(rq.at[1:8], 5).wait_recv()
    q = jnp.sum(rq[...].astype(F32), axis=0).reshape(16, 128).astype(BF16)
    loads[10].wait()
    tok = iota((16, 1024), 0) % 4
    scores = jnp.zeros((16, 1024), F32)
    for t in range(4):
        scores = jnp.where(tok == t, dot(q, k_v[t], NT), scores)
    scores = scores * (128.0 ** -0.5) + bias
    soft = jnp.log1p(jnp.exp(-jnp.abs(scores)))
    log_stop = jnp.minimum(scores, 0.0) - soft
    visible = iota((16, 1024), 1) < length
    log_keep = jnp.where(visible, log_stop - scores, 0.0)
    stacked = jnp.concatenate([log_keep[:, 128 * k : 128 * k + 128] for k in range(8)], axis=0)
    within = dot(stacked, later, precision=lax.Precision.HIGHEST)
    carry_sum = jnp.zeros((16, 1), F32)
    weights = [None] * 8
    for k in reversed(range(8)):
        inner = within[16 * k : 16 * k + 16]
        keep_k = log_keep[:, 128 * k : 128 * k + 128]
        expo = jnp.exp(log_stop[:, 128 * k : 128 * k + 128] + (inner + carry_sum))
        weights[k] = jnp.where(visible[:, 128 * k : 128 * k + 128], expo, 0.0)
        carry_sum = carry_sum + (inner[:, 0:1] + keep_k[:, 0:1])
    weight = jnp.concatenate(weights, axis=1).astype(BF16)
    loads[11].wait()
    tok_o = iota((16, 128), 0) % 4
    heads = jnp.zeros((16, 128), F32)
    for t in range(4):
        heads = jnp.where(tok_o == t, dot(weight, v_v[t]), heads)
    so[...] = heads.astype(BF16)

    for dy in (2, 1, 3, 0):
        for i in (0, 1, 3, 2):
            if dy or i != 2:
                send((z_at((2 - i) % NZ), x, c, y_at(dy)), so, ro.at[4 * y + i], 6)
    ro[4 * y + 2] = so[...]

    all_of(rh.at[1:4], 2).wait_recv()
    all_of(wo_g.at[1:NSHORT], 7).wait_recv()
    all_of(ro.at[1:NZ], 6).wait_recv()
    head_row = (iota((64, 128), 0) % 16) // 4
    resid = rh[...].astype(F32)
    for p in range(NY):
        heads_in = ro[4 * p : 4 * p + 4].reshape(64, 128)
        wo_p = wo_g[NXC * p : NXC * p + NXC].reshape(128, 512)
        proj = jnp.zeros((64, 128), F32)
        for h in range(4):
            proj = jnp.where(head_row == h, dot(heads_in, wo_p[:, 128 * h : 128 * h + 128], NT), proj)
        proj = jnp.sum(proj.reshape(4, 2, 8, 128), axis=1)
        proj = proj + pltpu.roll(proj, 4, 1)
        resid = resid + proj.astype(BF16).astype(F32)
    sd[...] = jnp.concatenate(
        [jnp.where(first8, resid[0], resid[1]), jnp.where(first8, resid[2], resid[3])], axis=0
    ).astype(BF16)

    for off in Z_ORDER:
        send((z_at(off), x, c, y), sd, rd.at[z], 8)
    rd[z] = sd[...]

    all_of(rr.at[1:NZ], 3).wait_recv()
    route = jnp.sum(rr[...].astype(F32), axis=0)

    groups = ((0, 4), (4, 4), (8, 8))

    def select_of(start, count, base, size):
        shape = (64, 16 * count)
        row = iota(shape, 0)
        expert = (NXC * z + row // 8).astype(F32)
        same = iota(shape, 1) // 4 + (start - 2) == base + row % size
        own = pltpu.roll(route, (4 * (2 - start)) % 128, 1)
        wanted = (own[0:1, 0 : 16 * count] == expert) | (own[1:2, 0 : 16 * count] == expert)
        return jnp.where(same & wanted, 1.0, 0.0).astype(BF16)

    def holders(base, size):
        counts = (3, 3, 2, 3) if size == 8 else (2, 2, 1, 2)
        return tuple((base + off, count) for off, count in zip((0, 1, 2, -1), counts))

    selects = [[select_of(*one, base, size) for one in holders(base, size)] for base, size in groups]

    def combine_of(base, size):
        rows, cols = (128, 64) if size == 8 else (64, 32)
        row = iota((rows, cols), 0)
        col = iota((rows, cols), 1)
        own = route[:, 8 * base : 8 * base + cols]
        if size == 8:
            expert, chunk, block = (row // 8) % NXC, row // 64, row % 8
        else:
            expert, chunk, block = row // 8, (row // 4) % 2, row % 4
        expert = (NXC * z + expert).astype(F32)
        same = (block == col // 8) & (chunk == (col // 4) % 2)
        weight = jnp.where(own[2:3] == expert, own[4:5], 0.0) + jnp.where(own[3:4] == expert, own[5:6], 0.0)
        return jnp.where(same, weight, 0.0).astype(BF16)

    combines = [combine_of(base, size) for base, size in groups]
    first64 = (iota((64, 128), 0) % 8) < 4
    first_ff = (iota((64, 192), 0) % 8) < 4
    bufs = ((sx4.at[0], rx4.at[0], se4.at[0], re4.at[0]), (sx4.at[1], rx4.at[1], se4.at[1], re4.at[1]), (sx, rx, se, re))

    def swap(v):
        return pltpu.roll(v.reshape(8, 8, v.shape[1]), 4, 1).reshape(v.shape)

    def to_experts(n, phase):
        out, into = bufs[n][0], bufs[n][1]
        base, size = groups[n]
        slots = []
        for k, (start, count) in enumerate(holders(base, size)):
            rows = jnp.concatenate([rd[(start + 4 * i) % NZ] for i in range(count)], axis=0)
            slots.append(dot(selects[n][k], rows))
        if size == 4:
            slots = [jnp.where(first64, slots[0], slots[1]), jnp.where(first64, slots[2], slots[3])]
        for k, slot in enumerate(slots):
            out[:, k] = slot.reshape(NXC, 8, 128).astype(BF16)
        for dx, dc, dy in SHORT_ORDER:
            px, pc = xc_at(dx, dc)
            send((z, px, pc, y_at(dy)), out.at[px * NC + pc], into.at[me], phase)
        into[me] = out[xc]

    all_of(rd.at[1:NZ], 8).wait_recv()
    to_experts(0, 9)
    to_experts(1, 17)
    to_experts(2, 13)

    pieces = [rd[z_at(18 - i)].astype(F32)[4 * i : 4 * i + 4] for i in range(4)]
    own_rows = []
    for k in range(4):
        row = jnp.zeros((4, 128), F32)
        for i in range(4):
            row = jnp.where(lax.rem(z + 18 - i, 4) == k, pieces[i], row)
        own_rows.append(row)

    def experts(n, phase):
        _, into, out, back = bufs[n]
        small = groups[n][1] == 4
        tiles = 2 if small else 4
        slots = into.reshape(NXC, NY, tiles, 8, 128)
        chunks = [slots[:, k // tiles, k % tiles].astype(F32).reshape(64, 128) for k in range(NY * tiles)]
        square = chunks[0] * chunks[0]
        for chunk in chunks[1:]:
            square = square + chunk * chunk
        if small:
            square = square + swap(square)
        scale_two = lax.rsqrt(jnp.sum(square, axis=-1, keepdims=True) * (1.0 / 2048.0) + EPS)

        def gain(k):
            if small:
                return jnp.where(first64, mgain_ref[2 * k : 2 * k + 1, :], mgain_ref[2 * k + 1 : 2 * k + 2, :])
            return mgain_ref[k : k + 1, :]

        lhs = jnp.concatenate([(one * scale_two * gain(k)).astype(BF16) for k, one in enumerate(chunks)], axis=1)

        def product(w):
            if not small:
                return dot(lhs, w[...], NT)
            even, odd = [
                dot(lhs, jnp.concatenate([w[:, 256 * k + o : 256 * k + o + 128] for k in range(8)], axis=1), NT)
                for o in (0, 128)
            ]
            both = jnp.where(first_ff, even, odd)
            return both + swap(both)

        gated = product(wg_v)
        upped = product(wu_v)
        act = (gated / (1.0 + jnp.exp(-gated)) * upped).astype(BF16)
        for p in range(NY):
            down = dot(act, wd_v[:, 512 * p : 512 * p + 512])
            parts = [down[:, 128 * k : 128 * k + 128] for k in range(4)]
            if small:
                parts = [jnp.where(first64, parts[0], parts[1]), jnp.where(first64, parts[2], parts[3])]
            for k, part in enumerate(parts):
                out[:, p, k] = part.reshape(NXC, 8, 128).astype(BF16)
        for dx, dc, dy in SHORT_ORDER:
            px, pc = xc_at(dx, dc)
            p = y_at(dy)
            send((z, px, pc, p), out.at[px * NC + pc, p], back.at[me], phase)
        back[me] = out[xc, y]

    def to_tokens(n):
        base, size = groups[n]
        tiles = 2 if size == 4 else 4
        parts = bufs[n][3].reshape(NXC, NY, tiles, 8, 128)
        totals = []
        for k in range(tiles):
            total = parts[:, 0, k].astype(F32)
            for p in range(1, NY):
                total = total + parts[:, p, k].astype(F32)
            totals.append(total.reshape(64, 128).astype(BF16))
        if size == 8:
            totals = [jnp.concatenate(totals[2 * p : 2 * p + 2], axis=0) for p in range(2)]
        for p in range(2):
            sf[base : base + size, p] = dot(combines[n], totals[p], TN).reshape(size, 8, 128).astype(BF16)

        def back(j):
            b = base + lax.rem(z + j, size)
            send((b, x, c, y), sf.at[b], rf.at[z], 11)

        @pl.when(lax.div(z, size) != base // size)
        def _():
            back(0)

        for j in range(1, size):
            back(j)

    for one in loads[12:]:
        one.wait()
    all_of(rx4.at[0, 1:NSHORT], 9).wait_recv()
    experts(0, 10)
    all_of(rx4.at[1, 1:NSHORT], 17).wait_recv()
    experts(1, 18)
    all_of(rx.at[1:NSHORT], 13).wait_recv()
    experts(2, 14)
    all_of(re4.at[0, 1:NSHORT], 10).wait_recv()
    to_tokens(0)
    all_of(re4.at[1, 1:NSHORT], 18).wait_recv()
    to_tokens(1)
    all_of(re.at[1:NSHORT], 14).wait_recv()
    to_tokens(2)
    rf[z] = sf[z]

    all_of(rf.at[1:NZ], 11).wait_recv()
    routed = jnp.sum(rf[...].astype(F32), axis=0).reshape(16, 128)
    for k in range(4):
        out_ref[:, 128 * k : 128 * k + 128] = (own_rows[k] + routed[4 * k : 4 * k + 4]).astype(BF16)

    for ref, phase in (
        (rn.at[1:8], 0),
        (wq_r.at[0], 1),
        (wq_r.at[0], 12),
        (rh.at[1:4], 2),
        (rr.at[1:NZ], 3),
        (wo_r.at[0:2], 4),
        (rq.at[1:8], 5),
        (ro.at[1:NZ], 6),
        (wo_g.at[1:NSHORT], 7),
        (rd.at[1:NZ], 8),
        (rx4.at[0, 1:NSHORT], 9),
        (rx4.at[1, 1:NSHORT], 17),
        (re4.at[1, 1:NSHORT], 18),
        (re4.at[0, 1:NSHORT], 10),
        (rf.at[1:NZ], 11),
        (rx.at[1:NSHORT], 13),
        (re.at[1:NSHORT], 14),
        (wq_g.at[1:NXC], 15),
        (wo_r.at[0:1], 16),
    ):
        all_of(ref, phase).wait_send()


def body(
    hidden,
    attn_gain,
    query_weight,
    head_bias,
    key_cache,
    value_cache,
    lengths,
    out_weight,
    moe_gain,
    route_group,
    route_inner,
    route_weight,
    gate_w,
    up_w,
    down_w,
):
    vmem = pl.BlockSpec(memory_space=pltpu.VMEM)
    hbm = pl.BlockSpec(memory_space=pltpu.HBM)

    def buf(*shape):
        return pltpu.VMEM(shape, BF16)

    return pl.pallas_call(
        kernel,
        out_shape=pltpu.VMEM((4, 512), BF16),
        in_specs=[hbm] * 15,
        out_specs=vmem,
        scratch_shapes=[
            buf(4, 2048),
            pltpu.VMEM((16, 128), F32),
            buf(16, 512),
            pltpu.SMEM((16,), F32),
            pltpu.SMEM((4,), jnp.int32),
            buf(16, 512),
            pltpu.VMEM((16, 128), F32),
            pltpu.SMEM((4,), jnp.int32),
            pltpu.SMEM((2, 4), jnp.int32),
            buf(2, 4),
            buf(4, 1024, 128),
            buf(4, 1024, 128),
            buf(192, 2048),
            buf(192, 2048),
            buf(192, 2048),
            buf(2, 16, 512),
            buf(NXC, 2, 16, 512),
            buf(4, 16, 512),
            buf(NSHORT, 16, 512),
            buf(NZ, 8, 128),
            buf(8, 8, 128),
            buf(NZ, 8, 128),
            buf(8, 128),
            buf(8, 8, 128),
            buf(4, 8, 128),
            buf(NZ, 8, 128),
            buf(8, 2, 8, 128),
            buf(8, 2, 8, 128),
            buf(16, 128),
            buf(NZ, 16, 128),
            buf(16, 128),
            buf(NZ, 16, 128),
            buf(2, NXC, 2, 8, 128),
            buf(2, NSHORT, 2, 8, 128),
            buf(2, NXC, NY, 2, 8, 128),
            buf(2, NSHORT, 2, 8, 128),
            buf(NXC, 4, 8, 128),
            buf(NSHORT, 4, 8, 128),
            buf(NXC, NY, 4, 8, 128),
            buf(NSHORT, 4, 8, 128),
            buf(NZ, 2, 8, 128),
            buf(NZ, 2, 8, 128),
            pltpu.SemaphoreType.DMA((15,)),
            pltpu.SemaphoreType.DMA((19,)),
            pltpu.SemaphoreType.DMA((19,)),
            pltpu.SemaphoreType.REGULAR,
        ],
        compiler_params=pltpu.CompilerParams(
            collective_id=0, has_side_effects=True, vmem_limit_bytes=40 * 1024 * 1024
        ),
        name="layer",
    )(*[pltpu.with_memory_space_constraint(a, pltpu.HBM) for a in (
        hidden,
        attn_gain.reshape(16, 128),
        query_weight,
        head_bias,
        key_cache.reshape(4, 1024, 128),
        value_cache.reshape(4, 1024, 128),
        lengths,
        out_weight.T,
        moe_gain.reshape(16, 128),
        route_group,
        route_inner.T,
        route_weight.T,
        jnp.swapaxes(gate_w, 1, 2).reshape(192, 2048),
        jnp.swapaxes(up_w, 1, 2).reshape(192, 2048),
        down_w.reshape(192, 2048),
    )])


def solution(mesh):
    torus = Mesh(mesh.devices.reshape(NZ, NX, NC, NY), ("ep_0", "ep_1", "ep_2", "tp"))
    placed = (
        P(EP, None),
        P(),
        P(EP, "tp"),
        P(),
        P(EP, "tp", None, None),
        P(EP, "tp", None, None),
        P(EP),
        P("tp", EP),
        P(),
        P(EP),
        P(EP, None),
        P(EP, None),
        P(EP, None, "tp"),
        P(EP, None, "tp"),
        P(EP, "tp", None),
    )
    return jax.shard_map(body, mesh=torus, in_specs=placed, out_specs=P(EP, "tp"), check_vma=False)
```

```python
import jax
import jax.numpy as jnp
from jax import lax
from jax.experimental import pallas as pl
from jax.experimental.pallas import tpu as pltpu
from jax.sharding import Mesh
from jax.sharding import PartitionSpec as P

EP = ("ep_0", "ep_1", "ep_2")
MESH = pl.DeviceIdType.MESH
F32 = jnp.float32
BF16 = jnp.bfloat16
NZ, NX, NC, NY = 16, 4, 2, 4
NXC = NX * NC
NSHORT = NXC * NY
EPS = 1e-06

Z_ORDER = (8, 7, 9, 6, 10, 5, 11, 4, 12, 3, 13, 2, 14, 1, 15)
NEAR_ORDER = (4, 12, 3, 13, 2, 14, 1, 15)
HOPS = (0, 1, 2, 1)
XC_ORDER = sorted(((dx, dc) for dx in range(NX) for dc in range(NC) if dx or dc), key=lambda d: (-HOPS[d[0]], d))
SHORT_ORDER = sorted(
    ((dx, dc, dy) for dx in range(NX) for dc in range(NC) for dy in range(NY) if dx or dc or dy),
    key=lambda d: (-HOPS[d[0]] - HOPS[d[2]], d[1], d[0] % 2, d),
)

NT = (((1,), (1,)), ((), ()))
TN = (((0,), (0,)), ((), ()))


def dot(a, b, dims=None, precision=None):
    if dims is None:
        dims = (((1,), (0,)), ((), ()))
    return lax.dot_general(a, b, dims, precision=precision, preferred_element_type=F32)


def iota(shape, dim):
    return lax.broadcasted_iota(jnp.int32, shape, dim)


def kernel(
    hid_hbm,
    again_hbm,
    wq_hbm,
    bias_hbm,
    k_hbm,
    v_hbm,
    len_hbm,
    wo_hbm,
    mgain_hbm,
    rg_hbm,
    ri_hbm,
    rw_hbm,
    gate_hbm,
    up_hbm,
    down_hbm,
    out_ref,
    hid_ref,
    again_ref,
    wq_ref,
    bias_ref,
    len_ref,
    wo_t,
    mgain_ref,
    rg_ref,
    ri_ref,
    rw_ref,
    k_v,
    v_v,
    wg_v,
    wu_v,
    wd_v,
    wq_r,
    wq_g,
    wo_r,
    wo_g,
    sn,
    st,
    sh,
    sr,
    rn,
    rh,
    rr,
    sq,
    rq,
    so,
    ro,
    sd,
    rd,
    sx4,
    rx4,
    se4,
    re4,
    sx,
    rx,
    se,
    re,
    sf,
    rf,
    load_sem,
    send_sem,
    recv_sem,
    past_sem,
):
    z = lax.axis_index("ep_0")
    x = lax.axis_index("ep_1")
    c = lax.axis_index("ep_2")
    y = lax.axis_index("tp")
    xc = x * NC + c
    me = xc * NY + y

    def z_at(off):
        return lax.rem(z + off, NZ)

    def xc_at(dx, dc):
        return lax.rem(x + dx, NX), lax.rem(c + dc, NC)

    def y_at(dy):
        return lax.rem(y + dy, NY)

    barrier = pltpu.get_barrier_semaphore()

    def greet(device):
        pl.semaphore_signal(barrier, inc=1, device_id=device, device_id_type=MESH)

    for off in NEAR_ORDER:
        greet((z_at(off), x, c, y))
    for dx, dc in XC_ORDER:
        greet((z, *xc_at(dx, dc), y))
    for dy in range(1, NY):
        greet((z, x, c, y_at(dy)))
    greeted = len(NEAR_ORDER) + NXC - 1 + NY - 1

    copies = (
        (hid_hbm, hid_ref),
        (again_hbm, again_ref),
        (rw_hbm, rw_ref),
        (rg_hbm, rg_ref),
        (ri_hbm, ri_ref),
        (wq_hbm, wq_ref),
        (wo_hbm, wo_t),
        (bias_hbm, bias_ref),
        (len_hbm, len_ref),
        (mgain_hbm, mgain_ref),
        (k_hbm, k_v),
        (v_hbm, v_v),
        (gate_hbm, wg_v),
        (up_hbm, wu_v),
        (down_hbm, wd_v),
    )
    loads = [pltpu.make_async_copy(src, dst, load_sem.at[i]) for i, (src, dst) in enumerate(copies)]
    for one in loads:
        one.start()
    for one in loads[0:5]:
        one.wait()

    hid = hid_ref[...].astype(F32)
    scale = lax.rsqrt(jnp.mean(hid * hid, axis=-1, keepdims=True) + EPS)
    hid2 = jnp.concatenate([hid, hid], axis=0)
    scale2 = jnp.concatenate([scale, scale], axis=0)
    for k in range(NZ):
        part = hid2[:, 128 * k : 128 * k + 128]
        sn[k] = (part * scale2 * again_ref[k : k + 1, :]).astype(BF16)
        sh[k] = part.astype(BF16)
    first8 = iota((8, 128), 0) < 4
    for i in range(8):
        st[i] = jnp.where(first8, sn[z_at(i)].astype(F32), sn[z_at(i + 8)].astype(F32)).astype(BF16)

    lane = iota((1, 128), 1)
    tok_a = lane % 4
    near = (lane % 64) // 4 == z
    wide = lane // 8 == z
    route_w = rw_ref[...].astype(F32)
    rows = []
    for pattern in (near, wide):
        for k in range(2):
            row = jnp.zeros((1, 128), F32)
            for t in range(4):
                ident = (rg_ref[t] * 32 + ri_ref[k, t]).astype(F32)
                row = jnp.where(tok_a == t, ident, row)
            rows.append(jnp.where(pattern, row, 0.0))
    for k in range(2):
        row = jnp.zeros((1, 128), F32)
        for t in range(4):
            row = jnp.where(tok_a == t, route_w[k : k + 1, t : t + 1], row)
        rows.append(jnp.where(wide, row, 0.0))
    rowid = iota((8, 128), 0)
    packet = jnp.zeros((8, 128), F32)
    for k, row in enumerate(rows):
        packet = jnp.where(rowid == k, jnp.broadcast_to(row, (8, 128)), packet)
    sr[...] = packet.astype(BF16)

    for one in loads[5:10]:
        one.wait()
    pl.semaphore_wait(barrier, greeted)

    def send(device, src, dst, phase):
        pltpu.make_async_remote_copy(
            src_ref=src,
            dst_ref=dst,
            send_sem=send_sem.at[phase],
            recv_sem=recv_sem.at[phase],
            device_id=device,
            device_id_type=MESH,
        ).start()

    def all_of(ref, phase):
        return pltpu.make_async_remote_copy(
            src_ref=ref,
            dst_ref=ref,
            send_sem=send_sem.at[phase],
            recv_sem=recv_sem.at[phase],
            device_id=(z_at(1), x, c, y),
            device_id_type=MESH,
        )

    quad = lax.div(z, 4)

    def share(slot):
        source = wo_r.at[slot] if slot else wo_t
        p = lax.rem(quad + slot, NY)
        for dx, dc in XC_ORDER:
            send((z, *xc_at(dx, dc), p), source, wo_g.at[y * NXC + xc], 7)

        @pl.when(p != y)
        def _():
            send((z, x, c, p), source, wo_g.at[y * NXC + xc], 7)

        @pl.when(p == y)
        def _():
            wo_g[y * NXC + xc] = source[...]

    send((z_at(12), x, c, y), wq_ref, wq_r.at[0], 1)
    send((z_at(4), x, c, y), wq_ref, wq_r.at[1], 12)
    for i in (0, 1, 7, 2, 6, 3, 5):
        send((z_at((i - 4) % NZ), x, c, y), st.at[i], rn.at[i], 0)
    for slot, off in ((1, 12), (3, 4)):
        send((z_at(off), x, c, y), wo_t, wo_r.at[slot], 4)

    def near_chunk(off):
        return lax.rem(z + off, 4) + 4 * y

    for i in range(4):
        if i != 2:
            off = (2 - i) % NZ
            send((z_at(off), x, c, y), sh.at[near_chunk(off)], rh.at[i], 2)
    rn[4] = st[4]
    rr[0] = sr[...]
    rh[2] = sh[near_chunk(0)]
    for dx, dc in XC_ORDER:
        pl.semaphore_signal(past_sem, inc=1, device_id=(z, *xc_at(dx, dc), y), device_id_type=MESH)

    pl.semaphore_wait(past_sem, NXC - 1)
    share(0)
    def gather_rows(slot, phase):
        all_of(wq_r.at[0], phase).wait_recv()
        for dx, dc in XC_ORDER:
            send((z, *xc_at(dx, dc), y), wq_r.at[slot], wq_g.at[xc, slot], 15)

    @pl.when(lax.rem(quad, 2) == 0)
    def _():
        gather_rows(0, 1)
        gather_rows(1, 12)

    @pl.when(lax.rem(quad, 2) == 1)
    def _():
        gather_rows(1, 12)
        gather_rows(0, 1)

    wq_g[xc] = wq_r[...]
    all_of(wo_r.at[0:2], 4).wait_recv()
    send((z_at(12), x, c, y), wo_r.at[1], wo_r.at[2], 16)
    for off in Z_ORDER:
        send((z_at(off), x, c, y), sr, rr.at[NZ - off], 3)
    all_of(rn.at[1:8], 0).wait_recv()
    xin = rn[...].astype(F32).reshape(64, 128).astype(BF16)
    all_of(wq_g.at[1:NXC], 15).wait_recv()

    first_q = (iota((64, 512), 0) % 8) < 4
    part_q = jnp.where(
        first_q, dot(xin, wq_g[:, 0].reshape(128, 512)), dot(xin, wq_g[:, 1].reshape(128, 512))
    ).reshape(8, 8, 512)
    part_q = (part_q + pltpu.roll(part_q, 4, 1)).reshape(64, 512)
    first = first_q[:, 0:128]
    for p in range(2):
        pair = jnp.where(first, part_q[:, 256 * p : 256 * p + 128], part_q[:, 256 * p + 128 : 256 * p + 256])
        sq[:, p] = pair.reshape(8, 8, 128).astype(BF16)
    for i in (0, 1, 7, 2, 6, 3, 5):
        send((z_at((4 - i) % NZ), x, c, y), sq.at[i], rq.at[i], 5)
    rq[4] = sq[4]

    share(1)
    share(3)


    later = (iota((128, 128), 0) > iota((128, 128), 1)).astype(BF16)
    rowh = iota((16, 1), 0)
    bias = jnp.zeros((16, 1), F32)
    length = jnp.zeros((16, 1), jnp.int32)
    for h in range(4):
        bias = jnp.where(rowh // 4 == h, bias_ref[4 * y + h], bias)
        length = jnp.where(rowh % 4 == h, len_ref[h], length)

    all_of(wo_r.at[0:1], 16).wait_recv()
    share(2)
    all_of(rq.at[1:8], 5).wait_recv()
    q = jnp.sum(rq[...].astype(F32), axis=0).reshape(16, 128).astype(BF16)
    loads[10].wait()
    tok = iota((16, 1024), 0) % 4
    scores = jnp.zeros((16, 1024), F32)
    for t in range(4):
        scores = jnp.where(tok == t, dot(q, k_v[t], NT), scores)
    scores = scores * (128.0 ** -0.5) + bias
    soft = jnp.log1p(jnp.exp(-jnp.abs(scores)))
    log_stop = jnp.minimum(scores, 0.0) - soft
    visible = iota((16, 1024), 1) < length
    log_keep = jnp.where(visible, log_stop - scores, 0.0)
    stacked = jnp.concatenate([log_keep[:, 128 * k : 128 * k + 128] for k in range(8)], axis=0)
    high = stacked.astype(BF16)
    mid = (stacked - high.astype(F32)).astype(BF16)
    low = (stacked - high.astype(F32) - mid.astype(F32)).astype(BF16)
    within = dot(high, later) + dot(mid, later) + dot(low, later)
    carry_sum = jnp.zeros((16, 1), F32)
    weights = [None] * 8
    for k in reversed(range(8)):
        inner = within[16 * k : 16 * k + 16]
        keep_k = log_keep[:, 128 * k : 128 * k + 128]
        expo = jnp.exp(log_stop[:, 128 * k : 128 * k + 128] + (inner + carry_sum))
        weights[k] = jnp.where(visible[:, 128 * k : 128 * k + 128], expo, 0.0)
        carry_sum = carry_sum + (inner[:, 0:1] + keep_k[:, 0:1])
    weight = jnp.concatenate(weights, axis=1).astype(BF16)
    loads[11].wait()
    tok_o = iota((16, 128), 0) % 4
    heads = jnp.zeros((16, 128), F32)
    for t in range(4):
        heads = jnp.where(tok_o == t, dot(weight, v_v[t]), heads)
    so[...] = heads.astype(BF16)

    for dy in (2, 1, 3, 0):
        for i in (0, 1, 3, 2):
            if dy or i != 2:
                send((z_at((2 - i) % NZ), x, c, y_at(dy)), so, ro.at[4 * y + i], 6)
    ro[4 * y + 2] = so[...]

    all_of(rh.at[1:4], 2).wait_recv()
    all_of(wo_g.at[1:NSHORT], 7).wait_recv()
    all_of(ro.at[1:NZ], 6).wait_recv()
    head_row = (iota((64, 128), 0) % 16) // 4
    resid = rh[...].astype(F32)
    for p in range(NY):
        heads_in = ro[4 * p : 4 * p + 4].reshape(64, 128)
        wo_p = wo_g[NXC * p : NXC * p + NXC].reshape(128, 512)
        proj = jnp.zeros((64, 128), F32)
        for h in range(4):
            proj = jnp.where(head_row == h, dot(heads_in, wo_p[:, 128 * h : 128 * h + 128], NT), proj)
        proj = jnp.sum(proj.reshape(4, 2, 8, 128), axis=1)
        proj = proj + pltpu.roll(proj, 4, 1)
        resid = resid + proj.astype(BF16).astype(F32)
    sd[...] = jnp.concatenate(
        [jnp.where(first8, resid[0], resid[1]), jnp.where(first8, resid[2], resid[3])], axis=0
    ).astype(BF16)

    for off in Z_ORDER:
        send((z_at(off), x, c, y), sd, rd.at[z], 8)
    rd[z] = sd[...]

    all_of(rr.at[1:NZ], 3).wait_recv()
    route = jnp.sum(rr[...].astype(F32), axis=0)

    groups = ((0, 4), (4, 4), (8, 8))

    def select_of(start, count, base, size):
        shape = (64, 16 * count)
        row = iota(shape, 0)
        expert = (NXC * z + row // 8).astype(F32)
        same = iota(shape, 1) // 4 + (start - 2) == base + row % size
        own = pltpu.roll(route, (4 * (2 - start)) % 128, 1)
        wanted = (own[0:1, 0 : 16 * count] == expert) | (own[1:2, 0 : 16 * count] == expert)
        return jnp.where(same & wanted, 1.0, 0.0).astype(BF16)

    def holders(base, size):
        counts = (3, 3, 2, 3) if size == 8 else (2, 2, 1, 2)
        return tuple((base + off, count) for off, count in zip((0, 1, 2, -1), counts))

    selects = [[select_of(*one, base, size) for one in holders(base, size)] for base, size in groups]

    def combine_of(base, size):
        rows, cols = (128, 64) if size == 8 else (64, 32)
        row = iota((rows, cols), 0)
        col = iota((rows, cols), 1)
        own = route[:, 8 * base : 8 * base + cols]
        if size == 8:
            expert, chunk, block = (row // 8) % NXC, row // 64, row % 8
        else:
            expert, chunk, block = row // 8, (row // 4) % 2, row % 4
        expert = (NXC * z + expert).astype(F32)
        same = (block == col // 8) & (chunk == (col // 4) % 2)
        weight = jnp.where(own[2:3] == expert, own[4:5], 0.0) + jnp.where(own[3:4] == expert, own[5:6], 0.0)
        return jnp.where(same, weight, 0.0).astype(BF16)

    combines = [combine_of(base, size) for base, size in groups]
    first64 = (iota((64, 128), 0) % 8) < 4
    first_ff = (iota((64, 192), 0) % 8) < 4
    bufs = ((sx4.at[0], rx4.at[0], se4.at[0], re4.at[0]), (sx4.at[1], rx4.at[1], se4.at[1], re4.at[1]), (sx, rx, se, re))

    def swap(v):
        return pltpu.roll(v.reshape(8, 8, v.shape[1]), 4, 1).reshape(v.shape)

    def to_experts(n, phase):
        out, into = bufs[n][0], bufs[n][1]
        base, size = groups[n]
        slots = []
        for k, (start, count) in enumerate(holders(base, size)):
            rows = jnp.concatenate([rd[(start + 4 * i) % NZ] for i in range(count)], axis=0)
            slots.append(dot(selects[n][k], rows))
        if size == 4:
            slots = [jnp.where(first64, slots[0], slots[1]), jnp.where(first64, slots[2], slots[3])]
        for k, slot in enumerate(slots):
            out[:, k] = slot.reshape(NXC, 8, 128).astype(BF16)
        for dx, dc, dy in SHORT_ORDER:
            px, pc = xc_at(dx, dc)
            send((z, px, pc, y_at(dy)), out.at[px * NC + pc], into.at[me], phase)
        into[me] = out[xc]

    all_of(rd.at[1:NZ], 8).wait_recv()
    to_experts(0, 9)
    to_experts(1, 17)
    to_experts(2, 13)

    pieces = [rd[z_at(18 - i)].astype(F32)[4 * i : 4 * i + 4] for i in range(4)]
    own_rows = []
    for k in range(4):
        row = jnp.zeros((4, 128), F32)
        for i in range(4):
            row = jnp.where(lax.rem(z + 18 - i, 4) == k, pieces[i], row)
        own_rows.append(row)

    def experts(n, phase):
        _, into, out, back = bufs[n]
        small = groups[n][1] == 4
        tiles = 2 if small else 4
        slots = into.reshape(NXC, NY, tiles, 8, 128)
        chunks = [slots[:, k // tiles, k % tiles].astype(F32).reshape(64, 128) for k in range(NY * tiles)]
        square = chunks[0] * chunks[0]
        for chunk in chunks[1:]:
            square = square + chunk * chunk
        if small:
            square = square + swap(square)
        scale_two = lax.rsqrt(jnp.sum(square, axis=-1, keepdims=True) * (1.0 / 2048.0) + EPS)

        def gain(k):
            if small:
                return jnp.where(first64, mgain_ref[2 * k : 2 * k + 1, :], mgain_ref[2 * k + 1 : 2 * k + 2, :])
            return mgain_ref[k : k + 1, :]

        lhs = jnp.concatenate([(one * gain(k)).astype(BF16) for k, one in enumerate(chunks)], axis=1)

        def product(w):
            if not small:
                return dot(lhs, w[...], NT)
            even, odd = [
                dot(lhs, jnp.concatenate([w[:, 256 * k + o : 256 * k + o + 128] for k in range(8)], axis=1), NT)
                for o in (0, 128)
            ]
            both = jnp.where(first_ff, even, odd)
            return both + swap(both)

        gated = product(wg_v) * scale_two
        upped = product(wu_v) * scale_two
        act = (gated / (1.0 + jnp.exp(-gated)) * upped).astype(BF16)
        for p in range(NY):
            down = dot(act, wd_v[:, 512 * p : 512 * p + 512])
            parts = [down[:, 128 * k : 128 * k + 128] for k in range(4)]
            if small:
                parts = [jnp.where(first64, parts[0], parts[1]), jnp.where(first64, parts[2], parts[3])]
            for k, part in enumerate(parts):
                out[:, p, k] = part.reshape(NXC, 8, 128).astype(BF16)
        for dx, dc, dy in SHORT_ORDER:
            px, pc = xc_at(dx, dc)
            p = y_at(dy)
            send((z, px, pc, p), out.at[px * NC + pc, p], back.at[me], phase)
        back[me] = out[xc, y]

    def to_tokens(n):
        base, size = groups[n]
        tiles = 2 if size == 4 else 4
        parts = bufs[n][3].reshape(NXC, NY, tiles, 8, 128)
        totals = []
        for k in range(tiles):
            total = parts[:, 0, k].astype(F32)
            for p in range(1, NY):
                total = total + parts[:, p, k].astype(F32)
            totals.append(total.reshape(64, 128).astype(BF16))
        if size == 8:
            totals = [jnp.concatenate(totals[2 * p : 2 * p + 2], axis=0) for p in range(2)]
        for p in range(2):
            sf[base : base + size, p] = dot(combines[n], totals[p], TN).reshape(size, 8, 128).astype(BF16)

        def back(j):
            b = base + lax.rem(z + j, size)
            send((b, x, c, y), sf.at[b], rf.at[z], 11)

        @pl.when(lax.div(z, size) != base // size)
        def _():
            back(0)

        for j in range(1, size):
            back(j)

    for one in loads[12:]:
        one.wait()
    all_of(rx4.at[0, 1:NSHORT], 9).wait_recv()
    experts(0, 10)
    all_of(rx4.at[1, 1:NSHORT], 17).wait_recv()
    experts(1, 18)
    all_of(rx.at[1:NSHORT], 13).wait_recv()
    experts(2, 14)
    all_of(re4.at[0, 1:NSHORT], 10).wait_recv()
    to_tokens(0)
    all_of(re4.at[1, 1:NSHORT], 18).wait_recv()
    to_tokens(1)
    all_of(re.at[1:NSHORT], 14).wait_recv()
    to_tokens(2)
    rf[z] = sf[z]

    all_of(rf.at[1:NZ], 11).wait_recv()
    routed = jnp.sum(rf[...].astype(F32), axis=0).reshape(16, 128)
    for k in range(4):
        out_ref[:, 128 * k : 128 * k + 128] = (own_rows[k] + routed[4 * k : 4 * k + 4]).astype(BF16)

    for ref, phase in (
        (rn.at[1:8], 0),
        (wq_r.at[0], 1),
        (wq_r.at[0], 12),
        (rh.at[1:4], 2),
        (rr.at[1:NZ], 3),
        (wo_r.at[0:2], 4),
        (rq.at[1:8], 5),
        (ro.at[1:NZ], 6),
        (wo_g.at[1:NSHORT], 7),
        (rd.at[1:NZ], 8),
        (rx4.at[0, 1:NSHORT], 9),
        (rx4.at[1, 1:NSHORT], 17),
        (re4.at[1, 1:NSHORT], 18),
        (re4.at[0, 1:NSHORT], 10),
        (rf.at[1:NZ], 11),
        (rx.at[1:NSHORT], 13),
        (re.at[1:NSHORT], 14),
        (wq_g.at[1:NXC], 15),
        (wo_r.at[0:1], 16),
    ):
        all_of(ref, phase).wait_send()


def body(
    hidden,
    attn_gain,
    query_weight,
    head_bias,
    key_cache,
    value_cache,
    lengths,
    out_weight,
    moe_gain,
    route_group,
    route_inner,
    route_weight,
    gate_w,
    up_w,
    down_w,
):
    vmem = pl.BlockSpec(memory_space=pltpu.VMEM)
    hbm = pl.BlockSpec(memory_space=pltpu.HBM)

    def buf(*shape):
        return pltpu.VMEM(shape, BF16)

    return pl.pallas_call(
        kernel,
        out_shape=pltpu.VMEM((4, 512), BF16),
        in_specs=[hbm] * 15,
        out_specs=vmem,
        scratch_shapes=[
            buf(4, 2048),
            pltpu.VMEM((16, 128), F32),
            buf(16, 512),
            pltpu.SMEM((16,), F32),
            pltpu.SMEM((4,), jnp.int32),
            buf(16, 512),
            pltpu.VMEM((16, 128), F32),
            pltpu.SMEM((4,), jnp.int32),
            pltpu.SMEM((2, 4), jnp.int32),
            buf(2, 4),
            buf(4, 1024, 128),
            buf(4, 1024, 128),
            buf(192, 2048),
            buf(192, 2048),
            buf(192, 2048),
            buf(2, 16, 512),
            buf(NXC, 2, 16, 512),
            buf(4, 16, 512),
            buf(NSHORT, 16, 512),
            buf(NZ, 8, 128),
            buf(8, 8, 128),
            buf(NZ, 8, 128),
            buf(8, 128),
            buf(8, 8, 128),
            buf(4, 8, 128),
            buf(NZ, 8, 128),
            buf(8, 2, 8, 128),
            buf(8, 2, 8, 128),
            buf(16, 128),
            buf(NZ, 16, 128),
            buf(16, 128),
            buf(NZ, 16, 128),
            buf(2, NXC, 2, 8, 128),
            buf(2, NSHORT, 2, 8, 128),
            buf(2, NXC, NY, 2, 8, 128),
            buf(2, NSHORT, 2, 8, 128),
            buf(NXC, 4, 8, 128),
            buf(NSHORT, 4, 8, 128),
            buf(NXC, NY, 4, 8, 128),
            buf(NSHORT, 4, 8, 128),
            buf(NZ, 2, 8, 128),
            buf(NZ, 2, 8, 128),
            pltpu.SemaphoreType.DMA((15,)),
            pltpu.SemaphoreType.DMA((19,)),
            pltpu.SemaphoreType.DMA((19,)),
            pltpu.SemaphoreType.REGULAR,
        ],
        compiler_params=pltpu.CompilerParams(
            collective_id=0, has_side_effects=True, vmem_limit_bytes=40 * 1024 * 1024
        ),
        name="layer",
    )(*[pltpu.with_memory_space_constraint(a, pltpu.HBM) for a in (
        hidden,
        attn_gain.reshape(16, 128),
        query_weight,
        head_bias,
        key_cache.reshape(4, 1024, 128),
        value_cache.reshape(4, 1024, 128),
        lengths,
        out_weight.T,
        moe_gain.reshape(16, 128),
        route_group,
        route_inner.T,
        route_weight.T,
        jnp.swapaxes(gate_w, 1, 2).reshape(192, 2048),
        jnp.swapaxes(up_w, 1, 2).reshape(192, 2048),
        down_w.reshape(192, 2048),
    )])


def solution(mesh):
    torus = Mesh(mesh.devices.reshape(NZ, NX, NC, NY), ("ep_0", "ep_1", "ep_2", "tp"))
    placed = (
        P(EP, None),
        P(),
        P(EP, "tp"),
        P(),
        P(EP, "tp", None, None),
        P(EP, "tp", None, None),
        P(EP),
        P("tp", EP),
        P(),
        P(EP),
        P(EP, None),
        P(EP, None),
        P(EP, None, "tp"),
        P(EP, None, "tp"),
        P(EP, "tp", None),
    )
    return jax.shard_map(body, mesh=torus, in_specs=placed, out_specs=P(EP, "tp"), check_vma=False)
```
